256 devices in a mesh: fs: 32 (over z, x), tp: 8 (over y, core).
Axes of the slice: x: 4, y: 4, z: 8, core: 2. Of those that a mesh axis runs over, the one named last changes fastest.
Arguments:
- tokens: bfloat16 [32768, 2048], P('fs', 'tp'), may hold values from -6 to 6
- grad_out: bfloat16 [32768, 2048], P('fs', 'tp'), may hold values from -6 to 6
- norm_gain: float32 [2048], replicated, may hold values from 0.1 to 1.9
- gate_weight: bfloat16 [3072, 2048], P('tp', 'fs'), may hold values from -0.125 to 0.125
- up_weight: bfloat16 [3072, 2048], P('tp', 'fs'), may hold values from -0.125 to 0.125
- down_weight: bfloat16 [3072, 2048], P('tp', 'fs'), may hold values from -0.109375 to 0.109375
Outputs:
- grad_input: bfloat16 [32768, 2048], P('fs', 'tp')
- grad_gate: float32 [3072, 2048], P('tp', 'fs')
- grad_up: float32 [3072, 2048], P('tp', 'fs')
- grad_down: float32 [3072, 2048], P('tp', 'fs')
- row_squares: float32 [3, 3072], P(None, 'tp')
The draws below stay inside these ranges and needn't reach their ends.
All inputs are finite; a program needn't handle non-finite values.
Results may differ from the reference program's by a relative error of at most 0.015.
Values may be sent and summed in bfloat16 or wider, within the bound.
No kernel may reach another device: no remote copies, remote signals or barrier semaphores. Data moves between devices by JAX's collectives and lax.ppermute only.
A program may use at most 64 MiB of HBM per device.

```python
import jax
import jax.numpy as jnp
from jax import lax

D = 2048
FF = 3072
TOKENS = 32768
N_TP = 8


def with_spikes(drawn, rng, source, target, blocks, factor):
    owner, partner = [(jnp.arange(drawn.shape[dim]) // (drawn.shape[dim] // blocks)).reshape([-1 if axis == dim else 1 for axis in range(drawn.ndim)]) for dim in (source, target)]
    chosen = jax.random.permutation(rng, blocks)[partner]
    strong = (owner == chosen) | (owner == (partner + blocks // 2) % blocks)
    return jnp.where(strong, factor * drawn, drawn)


def levels(own_key, dims, split, least, top_value):
    level, own = 1.0, jax.random.fold_in(own_key, 6)
    for position, shards_of in split:
        heights = jnp.exp(jax.random.uniform(jax.random.fold_in(own, position), (shards_of,), jnp.float32, least / len(split), top_value / len(split)))
        level = level * jnp.repeat(heights, dims[position] // shards_of).reshape([-1 if axis == position else 1 for axis in range(len(dims))])
    return level


def noise(stream_key, dims, scale, reach, pieces=(), dtype=jnp.bfloat16):
    loudness = levels(stream_key, dims, pieces, -0.22, 0.18) if pieces else 1.0
    entries = jax.random.normal(stream_key, dims, jnp.float32) * scale * loudness
    return jnp.minimum(jnp.maximum(entries, -reach), reach).astype(dtype)


def bell_draw_with(stream_key, extent, spread, bound, split, heavy, dtype=jnp.bfloat16):
    entries = spread * jax.random.normal(stream_key, extent, jnp.float32)
    if split:
        entries = entries * levels(stream_key, extent, split, -0.22, 0.18)
    return jnp.clip(with_spikes(entries, jax.random.fold_in(stream_key, 3), *heavy), -bound, bound).astype(dtype)


def setup_inputs(seed: int = 0) -> dict:
    key_list = jax.random.split(jax.random.key(seed), 7)
    tokens = noise(key_list[0], (TOKENS, D), 1.0, 6.0, ((0, 32), (1, 8)))
    grad_out = bell_draw_with(key_list[1], (TOKENS, D), 1.0, 6.0, ((0, 32), (1, 8)), (0, 1, 32, 2.75))
    norm_gain = jnp.clip(1.0 + 0.18 * jax.random.normal(key_list[2], (D,), jnp.float32), 0.1, 1.9)
    gate_weight = noise(key_list[3], (FF, D), D ** -0.5, 0.125, ((0, 8), (1, 32)))
    up_weight = noise(key_list[4], (FF, D), D ** -0.5, 0.125, ((0, 8), (1, 32)))
    down_weight = noise(key_list[5], (FF, D), FF ** -0.5, 0.109375, ((0, 8), (1, 32)))
    return {"tokens": tokens, "grad_out": grad_out, "norm_gain": norm_gain, "gate_weight": gate_weight, "up_weight": up_weight, "down_weight": down_weight}


def rms_back(grad_rows, unit_rows, inv_rms, gain_rows):
    scaled = gain_rows * grad_rows
    inner = lax.optimization_barrier(jnp.mean(scaled * unit_rows, axis=-1, keepdims=True))
    return inv_rms * (scaled - unit_rows * inner)

def reference(tokens, grad_out, norm_gain, gate_weight, up_weight, down_weight):
    floated = tokens.astype(jnp.float32)
    inv_rms = lax.rsqrt(lax.optimization_barrier(jnp.mean(floated * floated, axis=-1, keepdims=True)) + 1e-06)
    unit_rows = floated * inv_rms
    gain_rows = norm_gain.astype(jnp.float32)[None, :]
    normed = (unit_rows * gain_rows).astype(jnp.bfloat16)
    gate_pre = jnp.dot(normed, gate_weight.T, preferred_element_type=jnp.float32)
    up_pre = jnp.dot(normed, up_weight.T, preferred_element_type=jnp.float32)
    sigma = jax.nn.sigmoid(gate_pre)
    active = gate_pre * sigma
    hidden = (active * up_pre).astype(jnp.bfloat16)
    grad_hidden = 0.5 * jnp.dot(grad_out, down_weight.T, preferred_element_type=jnp.float32)
    gate_grad_pre = (grad_hidden * up_pre * sigma * (1.0 + gate_pre * (1.0 - sigma))).astype(jnp.bfloat16)
    up_grad_pre = (grad_hidden * active).astype(jnp.bfloat16)
    factor = TOKENS ** (-0.5)
    grad_down = 0.5 * factor * jnp.dot(hidden.T, grad_out, preferred_element_type=jnp.float32)
    grad_gate = factor * jnp.dot(gate_grad_pre.T, normed, preferred_element_type=jnp.float32)
    grad_up = factor * jnp.dot(up_grad_pre.T, normed, preferred_element_type=jnp.float32)
    width = FF // N_TP
    total = jnp.zeros(tokens.shape, jnp.float32)
    for block in range(N_TP):
        lower = block * width
        upper = lower + width
        grad_rows = jnp.dot(gate_grad_pre[:, lower:upper], gate_weight[lower:upper], preferred_element_type=jnp.float32)
        grad_rows = grad_rows + jnp.dot(up_grad_pre[:, lower:upper], up_weight[lower:upper], preferred_element_type=jnp.float32)
        partial_k = rms_back(grad_rows, unit_rows, inv_rms, gain_rows).astype(jnp.bfloat16)
        total = total + partial_k.astype(jnp.float32)
    grad_input = (grad_out.astype(jnp.float32) + total).astype(jnp.bfloat16)
    row_squares = jnp.stack([lax.optimization_barrier(jnp.sum(grad_gate * grad_gate, axis=1)), lax.optimization_barrier(jnp.sum(grad_up * grad_up, axis=1)), lax.optimization_barrier(jnp.sum(grad_down * grad_down, axis=1))]) / D
    return (grad_input, grad_gate, grad_up, grad_down, row_squares)
```

```python
import jax
import jax.numpy as jnp
from jax import lax
from jax.sharding import Mesh
from jax.sharding import PartitionSpec as P

FS = ("z", "x")
TP = ("y", "c")
ORDER = [(dy, dc) for dc in (0, 1) for dy in (0, 1, 3, 2)]


def shift(x, axis, k):
    n = lax.axis_size(axis)
    return lax.ppermute(x, axis, [(i, (i + k) % n) for i in range(n)])


def contract(left, right, left_dim, right_dim):
    return lax.dot_general(
        left, right, (((left_dim,), (right_dim,)), ((), ())), preferred_element_type=jnp.float32
    )


def on_device(tokens, grad_out, norm_gain, gate_weight, up_weight, down_weight):
    z, x, y, c = (lax.axis_index(a) for a in ("z", "x", "y", "c"))
    nz, nx, ny = (lax.axis_size(a) for a in ("z", "x", "y"))
    rows, width = tokens.shape
    hid, cols = gate_weight.shape

    turned = jnp.concatenate([gate_weight, up_weight, down_weight], axis=0).T
    t_left = shift(tokens, "y", 1)
    t_right = shift(tokens, "y", -1)
    w_x = {0: turned, 3: shift(turned, "x", 1), 1: shift(turned, "x", -1), 2: shift(turned, "x", 2)}
    g_left = shift(grad_out, "y", 1)
    g_right = shift(grad_out, "y", -1)
    plane = jnp.concatenate([w_x[k] for k in range(nx)] * 2, axis=0)
    plane = lax.dynamic_slice_in_dim(plane, ((nx - x) % nx) * cols, nx * cols, 0)
    ring = {0: plane}
    fore = back = plane
    for s in range(1, 4):
        fore = shift(fore, "z", 1)
        back = shift(back, "z", -1)
        ring[nz - s] = fore
        ring[s] = back
    half = plane.shape[0] // 2
    ring[4] = jnp.concatenate([shift(fore[:half], "z", 1), shift(back[half:], "z", -1)], axis=0)
    rolled = jnp.concatenate([ring[k] for k in range(nz)], axis=0)

    t_far = shift(t_left, "y", 1)
    g_far = shift(g_right, "y", -1)
    t_mine = [tokens, t_right, t_left, t_far]
    g_mine = [grad_out, g_right, g_left, g_far]
    t_all = jnp.concatenate(t_mine + [shift(v, "c", 1) for v in t_mine], axis=1)
    g_all = jnp.concatenate(g_mine + [shift(v, "c", 1) for v in g_mine], axis=1)

    blocks = [((y + dy) % ny) * 2 + (c + dc) % 2 for dy, dc in ORDER]
    weights = jnp.concatenate(
        [lax.dynamic_slice_in_dim(rolled, ((b - z) % nz) * width, width, 0) for b in blocks], axis=0
    )
    gain_rows = jnp.concatenate(
        [lax.dynamic_slice_in_dim(norm_gain, b * width, width, 0) for b in blocks]
    )[None, :]
    both_w, gate_w, up_w, down_w = (
        weights[:, : 2 * hid],
        weights[:, :hid],
        weights[:, hid : 2 * hid],
        weights[:, 2 * hid :],
    )

    floated = t_all.astype(jnp.float32)
    inv_rms = lax.rsqrt(jnp.mean(floated * floated, axis=-1, keepdims=True) + 1e-06)
    unit_rows = floated * inv_rms
    normed = (unit_rows * gain_rows).astype(jnp.bfloat16)
    factor = (rows * lax.axis_size(FS)) ** (-0.5)
    gate_pre = contract(normed, gate_w, 1, 0)
    up_pre = contract(normed, up_w, 1, 0)
    sigma = jax.nn.sigmoid(gate_pre)
    active = gate_pre * sigma
    hidden = (active * up_pre).astype(jnp.bfloat16)

    def to_owner_x(term):
        parts = term.reshape(nz, nx, cols, hid)
        own = lax.dynamic_index_in_dim(parts, x, 1, False).astype(jnp.float32)
        for k in (1, 3, 2):
            piece = lax.dynamic_index_in_dim(parts, (x + k) % nx, 1, False)
            own = own + shift(piece, "x", k).astype(jnp.float32)
        return own.astype(jnp.bfloat16)

    slots = []
    for b in range(nz):
        dy, dc = (b // 2 - y) % ny, (b + c) % 2
        place = jnp.where(dy == 3, 2, jnp.where(dy == 2, 3, dy))
        slots.append(dc * 4 + place)

    def to_owner_z(summed):
        ordered = jnp.stack([lax.dynamic_index_in_dim(summed, s, 0, False) for s in slots])
        got = lax.all_to_all(ordered, "z", 0, 0, tiled=True)
        return jnp.sum(got.astype(jnp.float32), axis=0)

    term_down = (0.5 * factor * contract(g_all, hidden, 0, 0)).astype(jnp.bfloat16)
    x_down = to_owner_x(term_down)
    grad_hidden = 0.5 * contract(g_all, down_w, 1, 0)
    gate_grad_pre = (grad_hidden * up_pre * sigma * (1.0 + gate_pre * (1.0 - sigma))).astype(
        jnp.bfloat16
    )
    up_grad_pre = (grad_hidden * active).astype(jnp.bfloat16)
    term_gate = (factor * contract(normed, gate_grad_pre, 0, 0)).astype(jnp.bfloat16)
    x_gate = to_owner_x(term_gate)
    term_up = (factor * contract(normed, up_grad_pre, 0, 0)).astype(jnp.bfloat16)
    x_up = to_owner_x(term_up)
    grad_rows = contract(gate_grad_pre, gate_w, 1, 1) + contract(up_grad_pre, up_w, 1, 1)
    scaled = gain_rows * grad_rows
    inner = jnp.mean(scaled * unit_rows, axis=-1, keepdims=True)
    partial = (inv_rms * (scaled - unit_rows * inner)).astype(jnp.bfloat16)

    half_w = 4 * width
    pair = partial[:, :half_w].astype(jnp.float32) + shift(partial[:, half_w:], "c", 1).astype(
        jnp.float32
    )
    total = grad_out.astype(jnp.float32) + pair[:, :width]
    for i, (dy, _) in enumerate(ORDER[1:4], start=1):
        piece = pair[:, i * width : (i + 1) * width].astype(jnp.bfloat16)
        total = total + shift(piece, "y", dy).astype(jnp.float32)
    grad_input = total.astype(jnp.bfloat16)

    grad_down, grad_gate, grad_up = to_owner_z(x_down), to_owner_z(x_gate), to_owner_z(x_up)
    squares = jnp.concatenate([jnp.sum(g * g, axis=0) for g in (grad_gate, grad_up, grad_down)])
    peers = nz * nx
    spread = jnp.broadcast_to(squares[None], (peers, squares.size))
    everything = lax.all_to_all(spread, FS, 0, 0, tiled=True)
    row_squares = jnp.sum(everything, axis=0).reshape(3, hid) / (cols * peers)
    return (grad_input, grad_gate.T, grad_up.T, grad_down.T, row_squares)


def solution(mesh):
    split = Mesh(mesh.devices.reshape(8, 4, 4, 2), ("z", "x", "y", "c"))
    return jax.shard_map(
        on_device,
        mesh=split,
        in_specs=(P(FS, TP), P(FS, TP), P(), P(TP, FS), P(TP, FS), P(TP, FS)),
        out_specs=(P(FS, TP), P(TP, FS), P(TP, FS), P(TP, FS), P(None, TP)),
        check_vma=False,
    )
```

```python
import jax
import jax.numpy as jnp
from jax import lax
from jax.experimental import pallas as pl
from jax.experimental.pallas import tpu as pltpu
from jax.sharding import Mesh
from jax.sharding import PartitionSpec as P

FS = ("z", "x")
TP = ("y", "c")
NZ, NX, NY = 8, 4, 4
DISTANCES = (0, 1, 3, 2)
VMEM = pl.BlockSpec(memory_space=pltpu.VMEM)
SMEM = pl.BlockSpec(memory_space=pltpu.SMEM)


def shift(x, axis, k):
    n = lax.axis_size(axis)
    return lax.ppermute(x, axis, [(i, (i + k) % n) for i in range(n)])


def contract(left, right, left_dim, right_dim):
    return lax.dot_general(
        left, right, (((left_dim,), (right_dim,)), ((), ())), preferred_element_type=jnp.float32
    )


def local_kernel(body, out, ins, flops=1 << 20):
    size = sum(a.size * a.dtype.itemsize for a in ins[1:])
    return pl.pallas_call(
        body,
        out_shape=out,
        in_specs=[SMEM] + [VMEM] * (len(ins) - 1),
        out_specs=jax.tree.map(lambda _: VMEM, out),
        cost_estimate=pl.CostEstimate(flops=flops, bytes_accessed=2 * size, transcendentals=0),
        compiler_params=pltpu.CompilerParams(vmem_limit_bytes=4 << 20),
    )(*ins)


def place_rows(places, pieces):
    rows = sum(p.shape[0] for p in pieces)

    def body(at, *refs):
        out = refs[-1]
        for k, ref in enumerate(refs[:-1]):
            start = pl.multiple_of(at[k], 64)
            out[pl.ds(start, ref.shape[0]), :] = ref[...]

    out = jax.ShapeDtypeStruct((rows, pieces[0].shape[1]), pieces[0].dtype)
    return local_kernel(body, out, (places, *pieces))


def sum_over_x(table, terms, arrived):
    nz, _, cols, hid = terms[0].shape

    def body(at, *refs):
        out = refs[-1]
        n = len(terms)
        for b in range(nz):
            slot = at[b]
            for w in range(n):
                total = refs[w][slot, at[nz]].astype(jnp.float32)
                for k in range(3):
                    total += refs[n + 3 * w + k][slot].astype(jnp.float32)
                out[b, :, w * hid : (w + 1) * hid] = total.astype(out.dtype)

    out = jax.ShapeDtypeStruct((nz, cols, hid * len(terms)), terms[0].dtype)
    flat = [p for group in arrived for p in group]
    return local_kernel(body, out, (table, *terms, *flat))


def sum_over_z(table, got, hid):
    nz, cols, width = got.shape
    n = width // hid

    def body(at, ref, *outs):
        for w in range(n):
            lanes = slice(w * hid, (w + 1) * hid)
            total = ref[0, :, lanes].astype(jnp.float32)
            for b in range(1, nz):
                total += ref[b, :, lanes].astype(jnp.float32)
            outs[w][...] = total
            outs[n][0:1, lanes] = jnp.sum(total * total, axis=0, keepdims=True)

    out = tuple(jax.ShapeDtypeStruct((cols, hid), jnp.float32) for _ in range(n))
    out += (jax.ShapeDtypeStruct((1, width), jnp.float32),)
    return local_kernel(body, out, (table, got))


def on_device(tokens, grad_out, norm_gain, gate_weight, up_weight, down_weight):
    z, x, y, c = (lax.axis_index(a) for a in ("z", "x", "y", "c"))
    rows, width = tokens.shape
    hid, cols = gate_weight.shape
    eight, four = jnp.arange(NZ, dtype=jnp.int32), jnp.arange(NX, dtype=jnp.int32)

    def slot_of(block):
        dy = ((block >> 1) - y) & 3
        return (((block & 1) ^ c) << 2) + (dy ^ (dy >> 1))

    block_at = ((y + ((eight & 3) ^ ((eight & 3) >> 1))) & 3) * 2 + ((eight >> 2) ^ c)
    slots = slot_of(eight)

    turned = jnp.concatenate([gate_weight, up_weight, down_weight], axis=0).T
    from_x = [turned]
    for k in (1, 2, 3):
        from_x.append(shift(turned, "x", -k % NX))
    t_left, t_right = shift(tokens, "y", 1), shift(tokens, "y", 3)
    g_left, g_right = shift(grad_out, "y", 1), shift(grad_out, "y", 3)
    plane = place_rows(((x + four) & 3) * cols, from_x)
    height = plane.shape[0]
    fore = back = plane
    ring = [(0, plane)]
    for s in (1, 2, 3):
        fore, back = shift(fore, "z", 1), shift(back, "z", 7)
        ring += [(-s, fore), (s, back)]
    half = height // 2
    ring += [(4, shift(fore[:half], "z", 1)), (4, shift(back[half:], "z", 7))]
    ring_at = slot_of((z + jnp.array([d for d, _ in ring], jnp.int32)) & 7) * height
    ring_at = ring_at.at[-1].add(half)

    t_far, g_far = shift(t_left, "y", 1), shift(g_right, "y", 3)
    t_mine, g_mine = [tokens, t_right, t_left, t_far], [grad_out, g_right, g_left, g_far]
    t_all = jnp.concatenate(t_mine + [shift(v, "c", 1) for v in t_mine], axis=1)
    g_all = jnp.concatenate(g_mine + [shift(v, "c", 1) for v in g_mine], axis=1)
    weights = place_rows(ring_at, [p for _, p in ring])
    gate_w, up_w, down_w = (weights[:, k * hid : (k + 1) * hid] for k in range(3))
    gain_rows = jnp.take(norm_gain.reshape(NZ, width), block_at, axis=0).reshape(1, -1)

    floated = t_all.astype(jnp.float32)
    inv_rms = lax.rsqrt(jnp.mean(floated * floated, axis=-1, keepdims=True) + 1e-06)
    unit_rows = floated * inv_rms
    normed = (unit_rows * gain_rows).astype(jnp.bfloat16)
    factor = (rows * lax.axis_size(FS)) ** (-0.5)
    gate_pre = contract(normed, gate_w, 1, 0)
    up_pre = contract(normed, up_w, 1, 0)
    sigma = jax.nn.sigmoid(gate_pre)
    active = gate_pre * sigma
    hidden = (active * up_pre).astype(jnp.bfloat16)

    def to_x_peers(term):
        parts = term.reshape(NZ, NX, cols, hid)
        pieces = [lax.dynamic_index_in_dim(parts, (x + k) & 3, 1, False) for k in (1, 2, 3)]
        return parts, [shift(p, "x", k) for k, p in zip((1, 2, 3), pieces)]

    term_down = (0.5 * factor * contract(g_all, hidden, 0, 0)).astype(jnp.bfloat16)
    own_down, x_down = to_x_peers(term_down)
    grad_hidden = 0.5 * contract(g_all, down_w, 1, 0)
    gate_grad_pre = (grad_hidden * up_pre * sigma * (1.0 + gate_pre * (1.0 - sigma))).astype(
        jnp.bfloat16
    )
    up_grad_pre = (grad_hidden * active).astype(jnp.bfloat16)
    term_gate = (factor * contract(normed, gate_grad_pre, 0, 0)).astype(jnp.bfloat16)
    own_gate, x_gate = to_x_peers(term_gate)
    term_up = (factor * contract(normed, up_grad_pre, 0, 0)).astype(jnp.bfloat16)
    own_up, x_up = to_x_peers(term_up)

    grad_rows = contract(gate_grad_pre, gate_w, 1, 1) + contract(up_grad_pre, up_w, 1, 1)
    scaled = gain_rows * grad_rows
    inner = jnp.mean(scaled * unit_rows, axis=-1, keepdims=True)
    partial = (inv_rms * (scaled - unit_rows * inner)).astype(jnp.bfloat16)
    half_w = 4 * width
    across = shift(partial[:, half_w:], "c", 1)

    def pair(i):
        lanes = slice(i * width, (i + 1) * width)
        return partial[:, lanes].astype(jnp.float32) + across[:, lanes].astype(jnp.float32)

    total = grad_out.astype(jnp.float32) + pair(0)
    from_y = [shift(pair(i).astype(jnp.bfloat16), "y", DISTANCES[i]) for i in (1, 2, 3)]
    for piece in from_y:
        total = total + piece.astype(jnp.float32)
    grad_input = total.astype(jnp.bfloat16)

    table = jnp.concatenate([slots, x[None].astype(jnp.int32)])
    ordered = sum_over_x(table, (own_gate, own_up, own_down), (x_gate, x_up, x_down))
    got = lax.all_to_all(ordered, "z", 0, 0, tiled=True)
    grad_gate, grad_up, grad_down, squares = sum_over_z(table, got, hid)
    peers = NZ * NX
    spread = jnp.broadcast_to(squares[None], (peers, *squares.shape))
    everything = lax.all_to_all(spread, FS, 0, 0, tiled=True)
    row_squares = jnp.sum(everything, axis=0).reshape(3, hid) / (cols * peers)
    return (grad_input, grad_gate.T, grad_up.T, grad_down.T, row_squares)


def solution(mesh):
    split = Mesh(mesh.devices.reshape(NZ, NX, NY, 2), FS + TP)

    return jax.shard_map(
        on_device,
        mesh=split,
        in_specs=(P(FS, TP), P(FS, TP), P(), P(TP, FS), P(TP, FS), P(TP, FS)),
        out_specs=(P(FS, TP), P(TP, FS), P(TP, FS), P(TP, FS), P(None, TP)),
        check_vma=False,
    )
```

```python
import jax
import jax.numpy as jnp
from jax import lax
from jax.experimental import pallas as pl
from jax.experimental.pallas import tpu as pltpu
from jax.sharding import Mesh
from jax.sharding import PartitionSpec as P

FS = ("z", "x")
TP = ("y", "c")
NZ, NX, NY = 8, 4, 4
DISTANCES = (0, 1, 3, 2)
VMEM = pl.BlockSpec(memory_space=pltpu.VMEM)
SMEM = pl.BlockSpec(memory_space=pltpu.SMEM)


def shift(x, axis, k):
    n = lax.axis_size(axis)
    return lax.ppermute(x, axis, [(i, (i + k) % n) for i in range(n)])


def local_kernel(body, out, ins, flops=1 << 20, limit=4, scratch=()):
    size = sum(a.size * a.dtype.itemsize for a in ins[1:])
    return pl.pallas_call(
        body,
        out_shape=out,
        in_specs=[SMEM] + [VMEM] * (len(ins) - 1),
        out_specs=jax.tree.map(lambda _: VMEM, out),
        scratch_shapes=scratch,
        cost_estimate=pl.CostEstimate(flops=flops, bytes_accessed=2 * size, transcendentals=0),
        compiler_params=pltpu.CompilerParams(vmem_limit_bytes=limit << 20),
    )(*ins)


def place_rows(places, pieces):
    rows = sum(p.shape[0] for p in pieces)

    def body(at, *refs):
        out = refs[-1]
        for k, ref in enumerate(refs[:-1]):
            start = pl.multiple_of(at[k], 64)
            out[pl.ds(start, ref.shape[0]), :] = ref[...]

    out = jax.ShapeDtypeStruct((rows, pieces[0].shape[1]), pieces[0].dtype)
    return local_kernel(body, out, (places, *pieces))


def place_down(table, pieces):
    _, cols, hid = pieces[0].shape

    def body(at, *refs):
        def step(b, carry):
            for k in range(NX):
                first = at[b] * (NX * cols) + ((at[NZ] + k) & 3) * cols
                refs[-1][pl.ds(pl.multiple_of(first, cols), cols), :] = refs[k][b]
            return carry

        lax.fori_loop(0, NZ, step, 0)

    out = jax.ShapeDtypeStruct((NZ * NX * cols, hid), pieces[0].dtype)
    return local_kernel(body, out, (table, *pieces))


def ordered_gain(block_at, gain):
    blocks, width = gain.shape

    def body(at, ref, out):
        for r in range(blocks):
            out[:, r * width : (r + 1) * width] = ref[pl.ds(at[r], 1), :]

    out = jax.ShapeDtypeStruct((1, blocks * width), gain.dtype)
    return local_kernel(body, out, (block_at, gain))


def sum_over_x(table, terms):
    def body(at, *refs):
        for b in range(NZ):
            total = refs[0][at[b]].astype(jnp.float32)
            for ref in refs[1:-1]:
                total += ref[at[b]].astype(jnp.float32)
            refs[-1][b] = total.astype(refs[-1].dtype)

    out = jax.ShapeDtypeStruct(terms[0].shape, terms[0].dtype)
    return local_kernel(body, out, (table, *terms))


def weight_grads(table, left, right, cols, scale, by_z):
    width, hid = left.shape[1] // NZ, right.shape[1]

    def body(at, l_ref, r_ref, *refs):
        scratch = refs[-1]

        def block(r):
            lanes = pl.ds(pl.multiple_of(r * width, width), width)
            product = lax.dot_general(
                l_ref[:, lanes],
                r_ref[...],
                (((0,), (0,)), ((), ())),
                preferred_element_type=jnp.float32,
            )
            term = (scale * product).astype(jnp.bfloat16)
            if by_z:
                scratch[r] = term
            else:
                scratch[r & 1] = term
                for k in range(NX):
                    first = pl.multiple_of(((at[NZ] + k) & 3) * cols, cols)
                    refs[k][r] = scratch[r & 1, pl.ds(first, cols), :]

        def step(i, carry):
            block(2 * i)
            block(2 * i + 1)
            return carry

        lax.fori_loop(0, NZ // 2, step, 0)
        if by_z:
            for j in range(NZ):
                refs[j][...] = scratch[at[NZ + 1 + j]]

    if by_z:
        out = tuple(jax.ShapeDtypeStruct((width, hid), jnp.bfloat16) for _ in range(NZ))
        scratch = [pltpu.VMEM((NZ, width, hid), jnp.bfloat16)]
    else:
        out = tuple(jax.ShapeDtypeStruct((NZ, cols, hid), jnp.bfloat16) for _ in range(NX))
        scratch = [pltpu.VMEM((2, width, hid), jnp.bfloat16)]
    flops = 2 * left.size * hid
    return local_kernel(body, out, (table, left, right), flops, 12, scratch)


def stacked(pieces):
    counts = [p.shape[0] if p.ndim == 3 else 1 for p in pieces]

    def body(at, *refs):
        place = 0
        for ref, n in zip(refs[:-1], counts):
            for k in range(n):
                refs[-1][place + k] = ref[k] if len(ref.shape) == 3 else ref[...]
            place += n

    out = jax.ShapeDtypeStruct((sum(counts), *pieces[0].shape[-2:]), pieces[0].dtype)
    return local_kernel(body, out, (jnp.zeros((1,), jnp.int32), *pieces), limit=6)


def block_rows(refs, kind, block, here):
    if block < 3:
        return refs[block][kind, here, :]
    if block == 3:
        return refs[3 + kind][here, :]
    if block < 7:
        return refs[5][(block - 4) * 2 + kind, here, :]
    return refs[6][kind, here, :]


TILE = 256


def forward(pieces, weights, down_w, gain_rows):
    rows, width = pieces[3].shape
    blocks = gain_rows.shape[1] // width
    hid = down_w.shape[1]

    def body(at, *refs):
        p_refs, (w_ref, d_ref, gain_ref) = refs[:7], refs[7:10]
        normed, g_all, inv_ref, hidden, pre_grads = refs[10:]

        def step(i, carry):
            start = pl.multiple_of(i * TILE, TILE)
            here = pl.ds(start, TILE)
            squares = jnp.zeros((TILE, width), jnp.float32)
            for r in range(blocks):
                t = block_rows(p_refs, 0, r, here).astype(jnp.float32)
                squares += t * t
            mean = jnp.sum(squares, axis=-1, keepdims=True) / (blocks * width)
            inv = lax.rsqrt(mean + 1e-06)
            inv_ref[here, :] = inv
            for r in range(blocks):
                lanes = slice(r * width, (r + 1) * width)
                t = block_rows(p_refs, 0, r, here).astype(jnp.float32)
                normed[here, lanes] = (t * inv * gain_ref[:, lanes]).astype(jnp.bfloat16)
                g_all[here, lanes] = block_rows(p_refs, 1, r, here)
            both = jnp.dot(normed[here, :], w_ref[...], preferred_element_type=jnp.float32)
            grad_hidden = 0.5 * jnp.dot(
                g_all[here, :], d_ref[...], preferred_element_type=jnp.float32
            )
            gate_pre, up_pre = both[:, :hid], both[:, hid:]
            sigma = jax.nn.sigmoid(gate_pre)
            active = gate_pre * sigma
            hidden[here, :] = (active * up_pre).astype(jnp.bfloat16)
            slope = sigma * (1.0 + gate_pre * (1.0 - sigma))
            pre_grads[here, :hid] = (grad_hidden * up_pre * slope).astype(jnp.bfloat16)
            pre_grads[here, hid:] = (grad_hidden * active).astype(jnp.bfloat16)
            return carry

        lax.fori_loop(0, rows // TILE, step, 0)

    half = jnp.bfloat16
    out = (
        jax.ShapeDtypeStruct((rows, blocks * width), half),
        jax.ShapeDtypeStruct((rows, blocks * width), half),
        jax.ShapeDtypeStruct((rows, 1), jnp.float32),
        jax.ShapeDtypeStruct((rows, hid), half),
        jax.ShapeDtypeStruct((rows, 2 * hid), half),
    )
    ins = (jnp.zeros((1,), jnp.int32), *pieces, weights, down_w, gain_rows)
    return local_kernel(body, out, ins, 5 * 10**9, 12)


def input_grads(pieces, inv_rms, gain_rows, pre_grads, weights):
    rows, width = pieces[3].shape
    blocks = gain_rows.shape[1] // width
    near = blocks // 2 * width

    def body(at, *refs):
        t_refs, (inv_ref, gain_ref, p_ref, w_ref) = refs[:7], refs[7:11]
        outs, acc = refs[11:13], refs[13]

        def step(i, carry):
            start = pl.multiple_of(i * TILE, TILE)
            here = pl.ds(start, TILE)
            acc[...] = lax.dot_general(
                p_ref[here, :],
                w_ref[...],
                (((1,), (1,)), ((), ())),
                preferred_element_type=jnp.float32,
            )
            inv = inv_ref[here, :]
            inner = jnp.zeros((TILE, width), jnp.float32)
            for r in range(blocks):
                lanes = slice(r * width, (r + 1) * width)
                unit = block_rows(t_refs, 0, r, here).astype(jnp.float32) * inv
                inner += gain_ref[:, lanes] * acc[:, lanes] * unit
            mean = jnp.sum(inner, axis=-1, keepdims=True) / (blocks * width)
            for r in range(blocks):
                lanes = slice(r * width, (r + 1) * width)
                unit = block_rows(t_refs, 0, r, here).astype(jnp.float32) * inv
                value = inv * (gain_ref[:, lanes] * acc[:, lanes] - unit * mean)
                place = slice(r % 4 * width, (r % 4 + 1) * width)
                outs[r // 4][here, place] = value.astype(jnp.bfloat16)
            return carry

        lax.fori_loop(0, rows // TILE, step, 0)

    out = tuple(jax.ShapeDtypeStruct((rows, near), jnp.bfloat16) for _ in range(2))
    ins = (jnp.zeros((1,), jnp.int32), *pieces, inv_rms, gain_rows, pre_grads, weights)
    scratch = [pltpu.VMEM((TILE, blocks * width), jnp.float32)]
    return local_kernel(body, out, ins, 3 * 10**9, 12, scratch)


def sum_for_x(table, terms, cols):
    hid = terms[0].shape[1]

    def body(at, *refs):
        outs = refs[NZ:]
        for k in range(NX):
            first = pl.multiple_of(((at[NZ] + k) & 3) * cols, cols)
            total = refs[0][pl.ds(first, cols), :].astype(jnp.float32)
            for ref in refs[1:NZ]:
                total += ref[pl.ds(first, cols), :].astype(jnp.float32)
            outs[k][...] = total.astype(outs[k].dtype)

    out = (jax.ShapeDtypeStruct((cols, hid), jnp.float32),)
    out += tuple(jax.ShapeDtypeStruct((cols, hid), terms[0].dtype) for _ in range(NX - 1))
    return local_kernel(body, out, (table, *terms))


def kernel(body, out, ins, specs, scratch=(), limit=4):
    size = sum(a.size * a.dtype.itemsize for a in ins)
    return pl.pallas_call(
        body,
        out_shape=out,
        in_specs=specs,
        out_specs=jax.tree.map(lambda _: VMEM, out),
        scratch_shapes=scratch,
        cost_estimate=pl.CostEstimate(flops=1 << 20, bytes_accessed=2 * size, transcendentals=0),
        compiler_params=pltpu.CompilerParams(vmem_limit_bytes=limit << 20),
    )(*ins)


def pair_sums(near, across, grad_out):
    rows, width = grad_out.shape

    def body(near_ref, across_ref, grad_ref, *outs):
        for i, out in enumerate(outs):
            lanes = slice(i * width, (i + 1) * width)
            both = near_ref[:, lanes].astype(jnp.float32) + across_ref[:, lanes].astype(jnp.float32)
            if i == 0:
                both += grad_ref[...].astype(jnp.float32)
            out[...] = both.astype(out.dtype)

    out = (jax.ShapeDtypeStruct((rows, width), jnp.float32),)
    out += tuple(jax.ShapeDtypeStruct((rows, width), jnp.bfloat16) for _ in range(3))
    return kernel(body, out, (near, across, grad_out), [VMEM] * 3, limit=12)


def final_sum(total, arrived):
    def body(total_ref, *refs):
        both = total_ref[...]
        for ref in refs[:-1]:
            both += ref[...].astype(jnp.float32)
        refs[-1][...] = both.astype(jnp.bfloat16)

    ins = (total, *arrived)
    out = jax.ShapeDtypeStruct(total.shape, jnp.bfloat16)
    return kernel(body, out, ins, [VMEM] * len(ins), limit=12)


def down_gradient(own, arrived):
    def body(own_ref, *refs):
        total = own_ref[...]
        for piece in refs[:-2]:
            total += piece[...].astype(jnp.float32)
        refs[-2][...] = total
        refs[-1][...] = jnp.sum(total * total, axis=0, keepdims=True)

    out = (
        jax.ShapeDtypeStruct(own.shape, jnp.float32),
        jax.ShapeDtypeStruct((1, own.shape[1]), jnp.float32),
    )
    ins = (own, *arrived)
    return kernel(body, out, ins, [VMEM] * len(ins))


def gradients(got, down_squares, peers):
    _, cols, both = got.shape
    hid = both // 2

    def body(ref, down_ref, gate, up, spread, line, sem):
        copy = pltpu.make_async_copy(down_ref, line.at[:, both:], sem)
        copy.start()
        for i, out in enumerate((gate, up)):
            lanes = slice(i * hid, (i + 1) * hid)
            total = ref[0, :, lanes].astype(jnp.float32)
            for b in range(1, NZ):
                total += ref[b, :, lanes].astype(jnp.float32)
            out[...] = total
            line[:, lanes] = jnp.sum(total * total, axis=0, keepdims=True)
        copy.wait()
        for k in range(peers):
            spread[k] = line[...]

    out = tuple(jax.ShapeDtypeStruct((cols, hid), jnp.float32) for _ in range(2))
    out += (jax.ShapeDtypeStruct((peers, 1, both + hid), jnp.float32),)
    specs = [VMEM, pl.BlockSpec(memory_space=pl.ANY)]
    scratch = [pltpu.VMEM((1, both + hid), jnp.float32), pltpu.SemaphoreType.DMA]
    return kernel(body, out, (got, down_squares), specs, scratch)


def mean_squares(everything, columns):
    peers, _, width = everything.shape
    hid = width // 3

    def body(ref, out):
        total = ref[0]
        for k in range(1, peers):
            total += ref[k]
        for i in range(3):
            out[i : i + 1, :] = total[:, i * hid : (i + 1) * hid] / columns

    out = jax.ShapeDtypeStruct((3, hid), jnp.float32)
    return kernel(body, out, (everything,), [VMEM])


def on_device(tokens, grad_out, norm_gain, gate_weight, up_weight, down_weight):
    z, x, y, c = (lax.axis_index(a) for a in ("z", "x", "y", "c"))
    rows, width = tokens.shape
    hid, cols = gate_weight.shape
    eight, four = jnp.arange(NZ, dtype=jnp.int32), jnp.arange(NX, dtype=jnp.int32)

    def slot_of(block):
        dy = ((block >> 1) - y) & 3
        return (((block & 1) ^ c) << 2) + (dy ^ (dy >> 1))

    block_at = ((y + ((eight & 3) ^ ((eight & 3) >> 1))) & 3) * 2 + ((eight >> 2) ^ c)
    slots = slot_of(eight)

    ring_steps = (0, -1, 1, -2, 2, -3, 3, 4, 4)
    height, half = NX * cols, NX * cols // 2
    ring_at = slot_of((z + jnp.array(ring_steps, jnp.int32)) & 7) * height
    ring_at = ring_at + jnp.array((0,) * 8 + (half,), jnp.int32)
    x_at = ((x + four) & 3) * cols
    table = jnp.concatenate([slots, x[None].astype(jnp.int32), slot_of((z + eight) & 7)])
    turned = jnp.concatenate([gate_weight, up_weight], axis=0).T
    down_own = jnp.broadcast_to(down_weight.T[None], (NZ, cols, hid))
    gain_table = norm_gain.reshape(NZ, width)
    gain_rows = ordered_gain(block_at, gain_table)
    ring_at, x_at, table, gain_rows, tokens, grad_out = lax.optimization_barrier(
        (ring_at, x_at, table, gain_rows, tokens, grad_out)
    )

    from_x = [turned]
    for k in (1, 2, 3):
        from_x.append(shift(turned, "x", -k % NX))
    mine = stacked((tokens, grad_out))
    left, right = shift(mine, "y", 1), shift(mine, "y", 3)
    down_z = lax.all_to_all(down_own, "z", 0, 0, tiled=True)
    from_x, down_z = lax.optimization_barrier((from_x, down_z))
    plane = place_rows(x_at, from_x)
    down_x = [shift(down_z, "x", -k % NX) for k in (1, 2, 3)]
    fore = back = plane
    ring = [plane]
    for _ in range(3):
        fore, back = shift(fore, "z", 1), shift(back, "z", 7)
        ring += [fore, back]
    ring += [shift(fore[:half], "z", 1), shift(back[half:], "z", 7)]

    t_near, g_near = left[0], right[1]
    t_far, g_far = shift(t_near, "y", 1), shift(g_near, "y", 3)
    across_near = shift(stacked((mine, right, left)), "c", 1)
    across_far = shift(stacked((t_far, g_far)), "c", 1)
    pieces = (mine, right, left, t_far, g_far, across_near, across_far)
    down_w = place_down(table, (down_z, *down_x))
    weights = place_rows(ring_at, ring)

    normed, g_all, inv_rms, hidden, pre_grads = forward(pieces, weights, down_w, gain_rows)
    factor = (rows * lax.axis_size(FS)) ** (-0.5)

    parts = weight_grads(table, normed, pre_grads, cols, factor, False)
    from_x = [shift(p, "x", k) for k, p in zip((1, 2, 3), parts[1:])]
    down = weight_grads(table, g_all, hidden, cols, 0.5 * factor, True)
    distances = (1, 7, 2, 6, 3, 5, 4)
    from_z = [shift(down[k], "z", k) for k in distances]
    near, far = input_grads(pieces, inv_rms, gain_rows, pre_grads, weights)
    across = shift(far, "c", 1)

    total, *to_y = pair_sums(near, across, grad_out)
    from_y = [shift(p, "y", DISTANCES[i]) for i, p in zip((1, 2, 3), to_y)]
    grad_input = final_sum(total, from_y)

    ordered = sum_over_x(table, (parts[0], *from_x))
    got_both = lax.all_to_all(ordered, "z", 0, 0, tiled=True)
    own_down, *for_x = sum_for_x(table, (down[0], *from_z), cols)
    x_down = [shift(p, "x", k) for k, p in zip((1, 2, 3), for_x)]
    peers = NZ * NX
    grad_down, down_squares = down_gradient(own_down, x_down)
    grad_gate, grad_up, spread = gradients(got_both, down_squares, peers)
    everything = lax.all_to_all(spread, FS, 0, 0, tiled=True)
    row_squares = mean_squares(everything, cols * peers)
    return (grad_input, grad_gate.T, grad_up.T, grad_down.T, row_squares)


def solution(mesh):
    split = Mesh(mesh.devices.reshape(NZ, NX, NY, 2), FS + TP)

    return jax.shard_map(
        on_device,
        mesh=split,
        in_specs=(P(FS, TP), P(FS, TP), P(), P(TP, FS), P(TP, FS), P(TP, FS)),
        out_specs=(P(FS, TP), P(TP, FS), P(TP, FS), P(TP, FS), P(None, TP)),
        check_vma=False,
    )
```

```python
import jax
import jax.numpy as jnp
from jax import lax
from jax.experimental import pallas as pl
from jax.experimental.pallas import tpu as pltpu
from jax.sharding import Mesh
from jax.sharding import PartitionSpec as P

FS = ("z", "x")
TP = ("y", "c")
NZ, NX, NY = 8, 4, 4
DISTANCES = (0, 1, 3, 2)
VMEM = pl.BlockSpec(memory_space=pltpu.VMEM)
SMEM = pl.BlockSpec(memory_space=pltpu.SMEM)


def shift(x, axis, k):
    n = lax.axis_size(axis)
    return lax.ppermute(x, axis, [(i, (i + k) % n) for i in range(n)])


def local_kernel(body, out, ins, flops=1 << 20, limit=4, scratch=()):
    size = sum(a.size * a.dtype.itemsize for a in ins[1:])
    return pl.pallas_call(
        body,
        out_shape=out,
        in_specs=[SMEM] + [VMEM] * (len(ins) - 1),
        out_specs=jax.tree.map(lambda _: VMEM, out),
        scratch_shapes=scratch,
        cost_estimate=pl.CostEstimate(flops=flops, bytes_accessed=2 * size, transcendentals=0),
        compiler_params=pltpu.CompilerParams(vmem_limit_bytes=limit << 20),
    )(*ins)


def place_rows(places, pieces):
    rows = sum(p.shape[0] for p in pieces)

    def body(at, *refs):
        out = refs[-1]
        for k, ref in enumerate(refs[:-1]):

            def step(i, carry, k=k, ref=ref):
                start = pl.multiple_of(at[k] + 32 * i, 32)
                out[pl.ds(start, 32), :] = ref[pl.ds(pl.multiple_of(32 * i, 32), 32), :]
                return carry

            lax.fori_loop(0, ref.shape[0] // 32, step, 0)

    out = jax.ShapeDtypeStruct((rows, pieces[0].shape[1]), pieces[0].dtype)
    return local_kernel(body, out, (places, *pieces))


def ordered_gain(block_at, gain):
    blocks, width = gain.shape

    def body(at, ref, out):
        for r in range(blocks):
            out[:, r * width : (r + 1) * width] = ref[pl.ds(at[r], 1), :]

    out = jax.ShapeDtypeStruct((1, blocks * width), gain.dtype)
    return local_kernel(body, out, (block_at, gain))


def sum_over_x(table, terms):
    n = len(terms)

    def body(at, *refs):
        def step(i, carry):
            here = pl.ds(pl.multiple_of(i * 16, 16), 16)
            for j in range(NZ):
                slot = at[NZ + 1 + j]
                total = refs[0][slot, here, :].astype(jnp.float32)
                for ref in refs[1:n]:
                    total += ref[slot, here, :].astype(jnp.float32)
                refs[n + j][here, :] = total.astype(refs[n + j].dtype)
            return carry

        lax.fori_loop(0, terms[0].shape[1] // 16, step, 0)

    out = jax.ShapeDtypeStruct(terms[0].shape[1:], terms[0].dtype)
    return local_kernel(body, (out,) * NZ, (table, *terms))


def weight_grads(table, left, right, cols, scale, by_z):
    width, hid = left.shape[1] // NZ, right.shape[1]

    def body(at, l_ref, r_ref, *refs):
        scratch = refs[-1]

        def block(r):
            lanes = pl.ds(pl.multiple_of(r * width, width), width)
            product = lax.dot_general(
                l_ref[:, lanes],
                r_ref[...],
                (((0,), (0,)), ((), ())),
                preferred_element_type=jnp.float32,
            )
            term = (scale * product).astype(jnp.bfloat16)
            if by_z:
                scratch[r] = term
            else:
                scratch[r & 1] = term
                for k in range(NX):
                    first = pl.multiple_of(((at[NZ] + k) & 3) * cols, cols)
                    refs[k][r] = scratch[r & 1, pl.ds(first, cols), :]

        together = 1 if by_z else 2

        def step(i, carry):
            for j in range(together):
                block(together * i + j)
            return carry

        lax.fori_loop(0, NZ // together, step, 0)
        if by_z:
            for j in range(NZ):
                refs[j][...] = scratch[at[NZ + 1 + j]]

    if by_z:
        out = tuple(jax.ShapeDtypeStruct((width, hid), jnp.bfloat16) for _ in range(NZ))
        scratch = [pltpu.VMEM((NZ, width, hid), jnp.bfloat16)]
    else:
        out = tuple(jax.ShapeDtypeStruct((NZ, cols, hid), jnp.bfloat16) for _ in range(NX))
        scratch = [pltpu.VMEM((2, width, hid), jnp.bfloat16)]
    flops = 2 * left.size * hid
    return local_kernel(body, out, (table, left, right), flops, 12, scratch)


def stacked(pieces):
    counts = [p.shape[0] if p.ndim == 3 else 1 for p in pieces]

    def body(at, *refs):
        place = 0
        for ref, n in zip(refs[:-1], counts):
            for k in range(n):
                refs[-1][place + k] = ref[k] if len(ref.shape) == 3 else ref[...]
            place += n

    out = jax.ShapeDtypeStruct((sum(counts), *pieces[0].shape[-2:]), pieces[0].dtype)
    return local_kernel(body, out, (jnp.zeros((1,), jnp.int32), *pieces), limit=6)


def block_rows(refs, kind, block, here):
    if block < 3:
        return refs[block][kind, here, :]
    if block == 3:
        return refs[3 + kind][here, :]
    if block < 7:
        return refs[5][(block - 4) * 2 + kind, here, :]
    return refs[6][kind, here, :]


TILE = 256


def forward(pieces, weights, gain_rows):
    rows, width = pieces[3].shape
    blocks = gain_rows.shape[1] // width
    hid = weights.shape[1] // 3

    def body(at, *refs):
        p_refs, (w_ref, gain_ref) = refs[:7], refs[7:9]
        normed, g_all, inv_ref, hidden, pre_grads = refs[9:]

        def step(i, carry):
            start = pl.multiple_of(i * TILE, TILE)
            here = pl.ds(start, TILE)
            squares = jnp.zeros((TILE, width), jnp.float32)
            for r in range(blocks):
                t = block_rows(p_refs, 0, r, here).astype(jnp.float32)
                squares += t * t
            mean = jnp.sum(squares, axis=-1, keepdims=True) / (blocks * width)
            inv = lax.rsqrt(mean + 1e-06)
            inv_ref[here, :] = inv
            for r in range(blocks):
                lanes = slice(r * width, (r + 1) * width)
                t = block_rows(p_refs, 0, r, here).astype(jnp.float32)
                normed[here, lanes] = (t * inv * gain_ref[:, lanes]).astype(jnp.bfloat16)
                g_all[here, lanes] = block_rows(p_refs, 1, r, here)
            both = jnp.dot(
                normed[here, :], w_ref[:, : 2 * hid], preferred_element_type=jnp.float32
            )
            grad_hidden = 0.5 * jnp.dot(
                g_all[here, :], w_ref[:, 2 * hid :], preferred_element_type=jnp.float32
            )
            gate_pre, up_pre = both[:, :hid], both[:, hid:]
            sigma = jax.nn.sigmoid(gate_pre)
            active = gate_pre * sigma
            hidden[here, :] = (active * up_pre).astype(jnp.bfloat16)
            slope = sigma * (1.0 + gate_pre * (1.0 - sigma))
            pre_grads[here, :hid] = (grad_hidden * up_pre * slope).astype(jnp.bfloat16)
            pre_grads[here, hid:] = (grad_hidden * active).astype(jnp.bfloat16)
            return carry

        lax.fori_loop(0, rows // TILE, step, 0)

    half = jnp.bfloat16
    out = (
        jax.ShapeDtypeStruct((rows, blocks * width), half),
        jax.ShapeDtypeStruct((rows, blocks * width), half),
        jax.ShapeDtypeStruct((rows, 1), jnp.float32),
        jax.ShapeDtypeStruct((rows, hid), half),
        jax.ShapeDtypeStruct((rows, 2 * hid), half),
    )
    ins = (jnp.zeros((1,), jnp.int32), *pieces, weights, gain_rows)
    return local_kernel(body, out, ins, 5 * 10**9, 12)


def input_grads(pieces, inv_rms, gain_rows, pre_grads, weights):
    rows, width = pieces[3].shape
    blocks = gain_rows.shape[1] // width
    both = pre_grads.shape[1]
    near = blocks // 2 * width

    def body(at, *refs):
        t_refs, (inv_ref, gain_ref, p_ref, w_ref) = refs[:7], refs[7:11]
        outs, acc = refs[11:13], refs[13]

        def step(i, carry):
            start = pl.multiple_of(i * TILE, TILE)
            here = pl.ds(start, TILE)
            acc[...] = lax.dot_general(
                p_ref[here, :],
                w_ref[:, :both],
                (((1,), (1,)), ((), ())),
                preferred_element_type=jnp.float32,
            )
            inv = inv_ref[here, :]
            inner = jnp.zeros((TILE, width), jnp.float32)
            for r in range(blocks):
                lanes = slice(r * width, (r + 1) * width)
                unit = block_rows(t_refs, 0, r, here).astype(jnp.float32) * inv
                inner += gain_ref[:, lanes] * acc[:, lanes] * unit
            mean = jnp.sum(inner, axis=-1, keepdims=True) / (blocks * width)
            for r in range(blocks):
                lanes = slice(r * width, (r + 1) * width)
                unit = block_rows(t_refs, 0, r, here).astype(jnp.float32) * inv
                value = inv * (gain_ref[:, lanes] * acc[:, lanes] - unit * mean)
                place = slice(r % 4 * width, (r % 4 + 1) * width)
                outs[r // 4][here, place] = value.astype(jnp.bfloat16)
            return carry

        lax.fori_loop(0, rows // TILE, step, 0)

    out = tuple(jax.ShapeDtypeStruct((rows, near), jnp.bfloat16) for _ in range(2))
    ins = (jnp.zeros((1,), jnp.int32), *pieces, inv_rms, gain_rows, pre_grads, weights)
    scratch = [pltpu.VMEM((TILE, blocks * width), jnp.float32)]
    return local_kernel(body, out, ins, 3 * 10**9, 12, scratch)


def sum_for_x(table, terms, cols):
    hid = terms[0].shape[1]

    def body(at, *refs):
        outs = refs[NZ:]

        def step(i, carry):
            here = pl.ds(pl.multiple_of(i * 16, 16), 16)
            for k in range(NX):
                first = pl.multiple_of(((at[NZ] + k) & 3) * cols + i * 16, 16)
                total = refs[0][pl.ds(first, 16), :].astype(jnp.float32)
                for ref in refs[1:NZ]:
                    total += ref[pl.ds(first, 16), :].astype(jnp.float32)
                outs[k][here, :] = total.astype(outs[k].dtype)
            return carry

        lax.fori_loop(0, cols // 16, step, 0)

    out = (jax.ShapeDtypeStruct((cols, hid), jnp.float32),)
    out += tuple(jax.ShapeDtypeStruct((cols, hid), terms[0].dtype) for _ in range(NX - 1))
    return local_kernel(body, out, (table, *terms))


def kernel(body, out, ins, specs, scratch=(), limit=4):
    size = sum(a.size * a.dtype.itemsize for a in ins)
    return pl.pallas_call(
        body,
        out_shape=out,
        in_specs=specs,
        out_specs=jax.tree.map(lambda _: VMEM, out),
        scratch_shapes=scratch,
        cost_estimate=pl.CostEstimate(flops=1 << 20, bytes_accessed=2 * size, transcendentals=0),
        compiler_params=pltpu.CompilerParams(vmem_limit_bytes=limit << 20),
    )(*ins)


def pair_sums(near, across, grad_out):
    rows, width = grad_out.shape

    def body(near_ref, across_ref, grad_ref, *outs):
        def step(n, carry):
            here = pl.ds(pl.multiple_of(n * TILE, TILE), TILE)
            for i, out in enumerate(outs):
                lanes = slice(i * width, (i + 1) * width)
                both = near_ref[here, lanes].astype(jnp.float32)
                both += across_ref[here, lanes].astype(jnp.float32)
                if i == 0:
                    both += grad_ref[here, :].astype(jnp.float32)
                out[here, :] = both.astype(out.dtype)
            return carry

        lax.fori_loop(0, rows // TILE, step, 0)

    out = (jax.ShapeDtypeStruct((rows, width), jnp.float32),)
    out += tuple(jax.ShapeDtypeStruct((rows, width), jnp.bfloat16) for _ in range(3))
    return kernel(body, out, (near, across, grad_out), [VMEM] * 3, limit=12)


def final_sum(total, arrived):
    def body(total_ref, *refs):
        def step(n, carry):
            here = pl.ds(pl.multiple_of(n * TILE, TILE), TILE)
            both = total_ref[here, :]
            for ref in refs[:-1]:
                both += ref[here, :].astype(jnp.float32)
            refs[-1][here, :] = both.astype(jnp.bfloat16)
            return carry

        lax.fori_loop(0, total.shape[0] // TILE, step, 0)

    ins = (total, *arrived)
    out = jax.ShapeDtypeStruct(total.shape, jnp.bfloat16)
    return kernel(body, out, ins, [VMEM] * len(ins), limit=12)


def down_gradient(own, arrived):
    def body(own_ref, *refs):
        total = own_ref[...]
        for piece in refs[:-2]:
            total += piece[...].astype(jnp.float32)
        refs[-2][...] = total
        refs[-1][...] = jnp.sum(total * total, axis=0, keepdims=True)

    out = (
        jax.ShapeDtypeStruct(own.shape, jnp.float32),
        jax.ShapeDtypeStruct((1, own.shape[1]), jnp.float32),
    )
    ins = (own, *arrived)
    return kernel(body, out, ins, [VMEM] * len(ins))


def gradients(terms, down_squares, peers):
    cols, both = terms[0].shape
    hid = both // 2

    def body(*refs):
        t_refs, down_ref, (gate, up, spread) = refs[:NZ], refs[NZ], refs[NZ + 1 : NZ + 4]
        line, sem = refs[NZ + 4 :]
        copy = pltpu.make_async_copy(down_ref, line.at[:, both:], sem)
        copy.start()
        for i, out in enumerate((gate, up)):
            lanes = slice(i * hid, (i + 1) * hid)
            total = t_refs[0][:, lanes].astype(jnp.float32)
            for ref in t_refs[1:]:
                total += ref[:, lanes].astype(jnp.float32)
            out[...] = total
            line[:, lanes] = jnp.sum(total * total, axis=0, keepdims=True)
        copy.wait()
        for k in range(peers):
            spread[k] = line[...]

    out = tuple(jax.ShapeDtypeStruct((cols, hid), jnp.float32) for _ in range(2))
    out += (jax.ShapeDtypeStruct((peers, 1, both + hid), jnp.float32),)
    specs = [VMEM] * NZ + [pl.BlockSpec(memory_space=pl.ANY)]
    scratch = [pltpu.VMEM((1, both + hid), jnp.float32), pltpu.SemaphoreType.DMA]
    return kernel(body, out, (*terms, down_squares), specs, scratch)


def mean_squares(everything, columns):
    peers, _, width = everything.shape
    hid = width // 3

    def body(ref, out):
        total = ref[0]
        for k in range(1, peers):
            total += ref[k]
        for i in range(3):
            out[i : i + 1, :] = total[:, i * hid : (i + 1) * hid] / columns

    out = jax.ShapeDtypeStruct((3, hid), jnp.float32)
    return kernel(body, out, (everything,), [VMEM])


def on_device(tokens, grad_out, norm_gain, gate_weight, up_weight, down_weight):
    z, x, y, c = (lax.axis_index(a) for a in ("z", "x", "y", "c"))
    rows, width = tokens.shape
    _, cols = gate_weight.shape
    eight, four = jnp.arange(NZ, dtype=jnp.int32), jnp.arange(NX, dtype=jnp.int32)

    def slot_of(block):
        dy = ((block >> 1) - y) & 3
        return (((block & 1) ^ c) << 2) + (dy ^ (dy >> 1))

    block_at = ((y + ((eight & 3) ^ ((eight & 3) >> 1))) & 3) * 2 + ((eight >> 2) ^ c)
    slots = slot_of(eight)

    ring_steps = (0, -1, 1, -2, 2, -3, 3, 4, 4)
    height, half = NX * cols, NX * cols // 2
    ring_at = slot_of((z + jnp.array(ring_steps, jnp.int32)) & 7) * height
    ring_at = ring_at + jnp.array((0,) * 8 + (half,), jnp.int32)
    x_at = ((x + four) & 3) * cols
    table = jnp.concatenate([slots, x[None].astype(jnp.int32), slot_of((z + eight) & 7)])
    turned = jnp.concatenate([gate_weight, up_weight, down_weight], axis=0).T
    gain_table = norm_gain.reshape(NZ, width)
    gain_rows = ordered_gain(block_at, gain_table)
    ring_at, x_at, table, gain_rows, tokens, grad_out = lax.optimization_barrier(
        (ring_at, x_at, table, gain_rows, tokens, grad_out)
    )

    from_x = [turned]
    for k in (1, 2, 3):
        from_x.append(shift(turned, "x", -k % NX))
    mine = stacked((tokens, grad_out))
    left, right = shift(mine, "y", 1), shift(mine, "y", 3)
    plane = place_rows(x_at, from_x)
    fore = back = plane
    ring = [plane]
    for _ in range(3):
        fore, back = shift(fore, "z", 1), shift(back, "z", 7)
        ring += [fore, back]
    ring += [shift(fore[:half], "z", 1), shift(back[half:], "z", 7)]

    t_near, g_near = left[0], right[1]
    t_far, g_far = shift(t_near, "y", 1), shift(g_near, "y", 3)
    across_near = shift(stacked((mine, right, left)), "c", 1)
    across_far = shift(stacked((t_far, g_far)), "c", 1)
    pieces = (mine, right, left, t_far, g_far, across_near, across_far)
    weights = place_rows(ring_at, ring)

    normed, g_all, inv_rms, hidden, pre_grads = forward(pieces, weights, gain_rows)
    factor = (rows * lax.axis_size(FS)) ** (-0.5)

    parts = weight_grads(table, normed, pre_grads, cols, factor, False)
    from_x = [shift(p, "x", k) for k, p in zip((1, 2, 3), parts[1:])]
    down = weight_grads(table, g_all, hidden, cols, 0.5 * factor, True)
    distances = (1, 7, 2, 6, 3, 5, 4)
    from_z = [shift(down[k], "z", k) for k in distances]
    near, far = input_grads(pieces, inv_rms, gain_rows, pre_grads, weights)
    across = shift(far, "c", 1)

    total, *to_y = pair_sums(near, across, grad_out)
    from_y = [shift(p, "y", DISTANCES[i]) for i, p in zip((1, 2, 3), to_y)]
    grad_input = final_sum(total, from_y)

    both_z = sum_over_x(table, (parts[0], *from_x))
    both_z = [both_z[0]] + [shift(both_z[k], "z", k) for k in distances]
    own_down, *for_x = sum_for_x(table, (down[0], *from_z), cols)
    x_down = [shift(p, "x", k) for k, p in zip((1, 2, 3), for_x)]
    peers = NZ * NX
    grad_down, down_squares = down_gradient(own_down, x_down)
    grad_gate, grad_up, spread = gradients(both_z, down_squares, peers)
    everything = lax.all_to_all(spread, FS, 0, 0, tiled=True)
    row_squares = mean_squares(everything, cols * peers)
    return (grad_input, grad_gate.T, grad_up.T, grad_down.T, row_squares)


def solution(mesh):
    split = Mesh(mesh.devices.reshape(NZ, NX, NY, 2), FS + TP)

    return jax.shard_map(
        on_device,
        mesh=split,
        in_specs=(P(FS, TP), P(FS, TP), P(), P(TP, FS), P(TP, FS), P(TP, FS)),
        out_specs=(P(FS, TP), P(TP, FS), P(TP, FS), P(TP, FS), P(None, TP)),
        check_vma=False,
    )
```

```python
import jax
import jax.numpy as jnp
from jax import lax
from jax.experimental import pallas as pl
from jax.experimental.pallas import tpu as pltpu
from jax.sharding import Mesh
from jax.sharding import PartitionSpec as P

FS = ("z", "x")
TP = ("y", "c")
NZ, NX, NY = 8, 4, 4
DISTANCES = (0, 1, 3, 2)
VMEM = pl.BlockSpec(memory_space=pltpu.VMEM)
SMEM = pl.BlockSpec(memory_space=pltpu.SMEM)


def shift(x, axis, k):
    n = lax.axis_size(axis)
    return lax.ppermute(x, axis, [(i, (i + k) % n) for i in range(n)])


def local_kernel(body, out, ins, flops=1 << 20, limit=4, scratch=()):
    size = sum(a.size * a.dtype.itemsize for a in ins[1:])
    return pl.pallas_call(
        body,
        out_shape=out,
        in_specs=[SMEM] + [VMEM] * (len(ins) - 1),
        out_specs=jax.tree.map(lambda _: VMEM, out),
        scratch_shapes=scratch,
        cost_estimate=pl.CostEstimate(flops=flops, bytes_accessed=2 * size, transcendentals=0),
        compiler_params=pltpu.CompilerParams(vmem_limit_bytes=limit << 20),
    )(*ins)


def place_rows(places, pieces):
    rows = sum(p.shape[0] for p in pieces)

    def body(at, *refs):
        out = refs[-1]
        for k, ref in enumerate(refs[:-1]):
            start = pl.multiple_of(at[k], 64)
            out[pl.ds(start, ref.shape[0]), :] = ref[...]

    out = jax.ShapeDtypeStruct((rows, pieces[0].shape[1]), pieces[0].dtype)
    return local_kernel(body, out, (places, *pieces))


def ordered_gain(block_at, gain):
    blocks, width = gain.shape

    def body(at, ref, out):
        for r in range(blocks):
            out[:, r * width : (r + 1) * width] = ref[pl.ds(at[r], 1), :]

    out = jax.ShapeDtypeStruct((1, blocks * width), gain.dtype)
    return local_kernel(body, out, (block_at, gain))


def sum_over_x(table, terms):
    def body(at, *refs):
        def step(i, carry):
            here = pl.ds(pl.multiple_of(i * 16, 16), 16)
            for b in range(NZ):
                total = refs[0][at[b], here, :].astype(jnp.float32)
                for ref in refs[1:-1]:
                    total += ref[at[b], here, :].astype(jnp.float32)
                refs[-1][b, here, :] = total.astype(refs[-1].dtype)
            return carry

        lax.fori_loop(0, terms[0].shape[1] // 16, step, 0)

    out = jax.ShapeDtypeStruct(terms[0].shape, terms[0].dtype)
    return local_kernel(body, out, (table, *terms))


def weight_grads(table, left, right, cols, scale, by_z):
    width, hid = left.shape[1] // NZ, right.shape[1]

    def body(at, l_ref, r_ref, *refs):
        scratch = refs[-1]

        def block(r):
            lanes = pl.ds(pl.multiple_of(r * width, width), width)
            product = lax.dot_general(
                l_ref[:, lanes],
                r_ref[...],
                (((0,), (0,)), ((), ())),
                preferred_element_type=jnp.float32,
            )
            term = (scale * product).astype(jnp.bfloat16)
            if by_z:
                scratch[r] = term
            else:
                scratch[r & 1] = term
                for k in range(NX):
                    first = pl.multiple_of(((at[NZ] + k) & 3) * cols, cols)
                    refs[k][r] = scratch[r & 1, pl.ds(first, cols), :]

        def step(i, carry):
            block(2 * i)
            block(2 * i + 1)
            return carry

        lax.fori_loop(0, NZ // 2, step, 0)
        if by_z:
            for j in range(NZ):
                refs[j][...] = scratch[at[NZ + 1 + j]]

    if by_z:
        out = tuple(jax.ShapeDtypeStruct((width, hid), jnp.bfloat16) for _ in range(NZ))
        scratch = [pltpu.VMEM((NZ, width, hid), jnp.bfloat16)]
    else:
        out = tuple(jax.ShapeDtypeStruct((NZ, cols, hid), jnp.bfloat16) for _ in range(NX))
        scratch = [pltpu.VMEM((2, width, hid), jnp.bfloat16)]
    flops = 2 * left.size * hid
    return local_kernel(body, out, (table, left, right), flops, 12, scratch)


def stacked(pieces):
    counts = [p.shape[0] if p.ndim == 3 else 1 for p in pieces]

    def body(at, *refs):
        place = 0
        for ref, n in zip(refs[:-1], counts):
            for k in range(n):
                refs[-1][place + k] = ref[k] if len(ref.shape) == 3 else ref[...]
            place += n

    out = jax.ShapeDtypeStruct((sum(counts), *pieces[0].shape[-2:]), pieces[0].dtype)
    return local_kernel(body, out, (jnp.zeros((1,), jnp.int32), *pieces), limit=6)


def block_rows(refs, kind, block, here):
    if block < 3:
        return refs[block][kind, here, :]
    if block == 3:
        return refs[3 + kind][here, :]
    if block < 7:
        return refs[5][(block - 4) * 2 + kind, here, :]
    return refs[6][kind, here, :]


TILE = 256


def forward(pieces, weights, gain_rows):
    rows, width = pieces[3].shape
    blocks = gain_rows.shape[1] // width
    hid = weights.shape[1] // 3

    def body(at, *refs):
        p_refs, (w_ref, gain_ref) = refs[:7], refs[7:9]
        normed, g_all, inv_ref, hidden, pre_grads = refs[9:]

        def step(i, carry):
            start = pl.multiple_of(i * TILE, TILE)
            here = pl.ds(start, TILE)
            squares = jnp.zeros((TILE, width), jnp.float32)
            for r in range(blocks):
                t = block_rows(p_refs, 0, r, here).astype(jnp.float32)
                squares += t * t
            mean = jnp.sum(squares, axis=-1, keepdims=True) / (blocks * width)
            inv = lax.rsqrt(mean + 1e-06)
            inv_ref[here, :] = inv
            for r in range(blocks):
                lanes = slice(r * width, (r + 1) * width)
                t = block_rows(p_refs, 0, r, here).astype(jnp.float32)
                normed[here, lanes] = (t * inv * gain_ref[:, lanes]).astype(jnp.bfloat16)
                g_all[here, lanes] = block_rows(p_refs, 1, r, here)
            both = jnp.dot(
                normed[here, :], w_ref[:, : 2 * hid], preferred_element_type=jnp.float32
            )
            grad_hidden = 0.5 * jnp.dot(
                g_all[here, :], w_ref[:, 2 * hid :], preferred_element_type=jnp.float32
            )
            gate_pre, up_pre = both[:, :hid], both[:, hid:]
            sigma = jax.nn.sigmoid(gate_pre)
            active = gate_pre * sigma
            hidden[here, :] = (active * up_pre).astype(jnp.bfloat16)
            slope = sigma * (1.0 + gate_pre * (1.0 - sigma))
            pre_grads[here, :hid] = (grad_hidden * up_pre * slope).astype(jnp.bfloat16)
            pre_grads[here, hid:] = (grad_hidden * active).astype(jnp.bfloat16)
            return carry

        lax.fori_loop(0, rows // TILE, step, 0)

    half = jnp.bfloat16
    out = (
        jax.ShapeDtypeStruct((rows, blocks * width), half),
        jax.ShapeDtypeStruct((rows, blocks * width), half),
        jax.ShapeDtypeStruct((rows, 1), jnp.float32),
        jax.ShapeDtypeStruct((rows, hid), half),
        jax.ShapeDtypeStruct((rows, 2 * hid), half),
    )
    ins = (jnp.zeros((1,), jnp.int32), *pieces, weights, gain_rows)
    return local_kernel(body, out, ins, 5 * 10**9, 12)


def input_grads(pieces, inv_rms, gain_rows, pre_grads, weights):
    rows, width = pieces[3].shape
    blocks = gain_rows.shape[1] // width
    both = pre_grads.shape[1]
    near = blocks // 2 * width

    def body(at, *refs):
        t_refs, (inv_ref, gain_ref, p_ref, w_ref) = refs[:7], refs[7:11]
        outs, acc = refs[11:13], refs[13]

        def step(i, carry):
            start = pl.multiple_of(i * TILE, TILE)
            here = pl.ds(start, TILE)
            acc[...] = lax.dot_general(
                p_ref[here, :],
                w_ref[:, :both],
                (((1,), (1,)), ((), ())),
                preferred_element_type=jnp.float32,
            )
            inv = inv_ref[here, :]
            inner = jnp.zeros((TILE, width), jnp.float32)
            for r in range(blocks):
                lanes = slice(r * width, (r + 1) * width)
                unit = block_rows(t_refs, 0, r, here).astype(jnp.float32) * inv
                inner += gain_ref[:, lanes] * acc[:, lanes] * unit
            mean = jnp.sum(inner, axis=-1, keepdims=True) / (blocks * width)
            for r in range(blocks):
                lanes = slice(r * width, (r + 1) * width)
                unit = block_rows(t_refs, 0, r, here).astype(jnp.float32) * inv
                value = inv * (gain_ref[:, lanes] * acc[:, lanes] - unit * mean)
                place = slice(r % 4 * width, (r % 4 + 1) * width)
                outs[r // 4][here, place] = value.astype(jnp.bfloat16)
            return carry

        lax.fori_loop(0, rows // TILE, step, 0)

    out = tuple(jax.ShapeDtypeStruct((rows, near), jnp.bfloat16) for _ in range(2))
    ins = (jnp.zeros((1,), jnp.int32), *pieces, inv_rms, gain_rows, pre_grads, weights)
    scratch = [pltpu.VMEM((TILE, blocks * width), jnp.float32)]
    return local_kernel(body, out, ins, 3 * 10**9, 12, scratch)


def sum_for_x(table, terms, cols):
    hid = terms[0].shape[1]

    def body(at, *refs):
        outs = refs[NZ:]

        def step(i, carry):
            here = pl.ds(pl.multiple_of(i * 16, 16), 16)
            for k in range(NX):
                first = pl.multiple_of(((at[NZ] + k) & 3) * cols + i * 16, 16)
                total = refs[0][pl.ds(first, 16), :].astype(jnp.float32)
                for ref in refs[1:NZ]:
                    total += ref[pl.ds(first, 16), :].astype(jnp.float32)
                outs[k][here, :] = total.astype(outs[k].dtype)
            return carry

        lax.fori_loop(0, cols // 16, step, 0)

    out = (jax.ShapeDtypeStruct((cols, hid), jnp.float32),)
    out += tuple(jax.ShapeDtypeStruct((cols, hid), terms[0].dtype) for _ in range(NX - 1))
    return local_kernel(body, out, (table, *terms))


def kernel(body, out, ins, specs, scratch=(), limit=4):
    size = sum(a.size * a.dtype.itemsize for a in ins)
    return pl.pallas_call(
        body,
        out_shape=out,
        in_specs=specs,
        out_specs=jax.tree.map(lambda _: VMEM, out),
        scratch_shapes=scratch,
        cost_estimate=pl.CostEstimate(flops=1 << 20, bytes_accessed=2 * size, transcendentals=0),
        compiler_params=pltpu.CompilerParams(vmem_limit_bytes=limit << 20),
    )(*ins)


def pair_sums(near, across, grad_out):
    rows, width = grad_out.shape

    def body(near_ref, across_ref, grad_ref, *outs):
        def step(n, carry):
            here = pl.ds(pl.multiple_of(n * TILE, TILE), TILE)
            for i, out in enumerate(outs):
                lanes = slice(i * width, (i + 1) * width)
                both = near_ref[here, lanes].astype(jnp.float32)
                both += across_ref[here, lanes].astype(jnp.float32)
                if i == 0:
                    both += grad_ref[here, :].astype(jnp.float32)
                out[here, :] = both.astype(out.dtype)
            return carry

        lax.fori_loop(0, rows // TILE, step, 0)

    out = (jax.ShapeDtypeStruct((rows, width), jnp.float32),)
    out += tuple(jax.ShapeDtypeStruct((rows, width), jnp.bfloat16) for _ in range(3))
    return kernel(body, out, (near, across, grad_out), [VMEM] * 3, limit=12)


def final_sum(total, arrived):
    def body(total_ref, *refs):
        def step(n, carry):
            here = pl.ds(pl.multiple_of(n * TILE, TILE), TILE)
            both = total_ref[here, :]
            for ref in refs[:-1]:
                both += ref[here, :].astype(jnp.float32)
            refs[-1][here, :] = both.astype(jnp.bfloat16)
            return carry

        lax.fori_loop(0, total.shape[0] // TILE, step, 0)

    ins = (total, *arrived)
    out = jax.ShapeDtypeStruct(total.shape, jnp.bfloat16)
    return kernel(body, out, ins, [VMEM] * len(ins), limit=12)


def down_gradient(own, arrived):
    def body(own_ref, *refs):
        total = own_ref[...]
        for piece in refs[:-2]:
            total += piece[...].astype(jnp.float32)
        refs[-2][...] = total
        refs[-1][...] = jnp.sum(total * total, axis=0, keepdims=True)

    out = (
        jax.ShapeDtypeStruct(own.shape, jnp.float32),
        jax.ShapeDtypeStruct((1, own.shape[1]), jnp.float32),
    )
    ins = (own, *arrived)
    return kernel(body, out, ins, [VMEM] * len(ins))


def gradients(got, down_squares, peers):
    _, cols, both = got.shape
    hid = both // 2

    def body(ref, down_ref, gate, up, spread, line, sem):
        copy = pltpu.make_async_copy(down_ref, line.at[:, both:], sem)
        copy.start()
        for i, out in enumerate((gate, up)):
            lanes = slice(i * hid, (i + 1) * hid)
            total = ref[0, :, lanes].astype(jnp.float32)
            for b in range(1, NZ):
                total += ref[b, :, lanes].astype(jnp.float32)
            out[...] = total
            line[:, lanes] = jnp.sum(total * total, axis=0, keepdims=True)
        copy.wait()
        for k in range(peers):
            spread[k] = line[...]

    out = tuple(jax.ShapeDtypeStruct((cols, hid), jnp.float32) for _ in range(2))
    out += (jax.ShapeDtypeStruct((peers, 1, both + hid), jnp.float32),)
    specs = [VMEM, pl.BlockSpec(memory_space=pl.ANY)]
    scratch = [pltpu.VMEM((1, both + hid), jnp.float32), pltpu.SemaphoreType.DMA]
    return kernel(body, out, (got, down_squares), specs, scratch)


def mean_squares(everything, columns):
    peers, _, width = everything.shape
    hid = width // 3

    def body(ref, out):
        total = ref[0]
        for k in range(1, peers):
            total += ref[k]
        for i in range(3):
            out[i : i + 1, :] = total[:, i * hid : (i + 1) * hid] / columns

    out = jax.ShapeDtypeStruct((3, hid), jnp.float32)
    return kernel(body, out, (everything,), [VMEM])


def on_device(tokens, grad_out, norm_gain, gate_weight, up_weight, down_weight):
    z, x, y, c = (lax.axis_index(a) for a in ("z", "x", "y", "c"))
    rows, width = tokens.shape
    _, cols = gate_weight.shape
    eight, four = jnp.arange(NZ, dtype=jnp.int32), jnp.arange(NX, dtype=jnp.int32)

    def slot_of(block):
        dy = ((block >> 1) - y) & 3
        return (((block & 1) ^ c) << 2) + (dy ^ (dy >> 1))

    block_at = ((y + ((eight & 3) ^ ((eight & 3) >> 1))) & 3) * 2 + ((eight >> 2) ^ c)
    slots = slot_of(eight)

    ring_steps = (0, -1, 1, -2, 2, -3, 3, 4, 4)
    height, half = NX * cols, NX * cols // 2
    ring_at = slot_of((z + jnp.array(ring_steps, jnp.int32)) & 7) * height
    ring_at = ring_at + jnp.array((0,) * 8 + (half,), jnp.int32)
    x_at = ((x + four) & 3) * cols
    table = jnp.concatenate([slots, x[None].astype(jnp.int32), slot_of((z + eight) & 7)])
    turned = jnp.concatenate([gate_weight, up_weight, down_weight], axis=0).T
    gain_table = norm_gain.reshape(NZ, width)
    gain_rows = ordered_gain(block_at, gain_table)
    ring_at, x_at, table, gain_rows, tokens, grad_out = lax.optimization_barrier(
        (ring_at, x_at, table, gain_rows, tokens, grad_out)
    )

    from_x = [turned]
    for k in (1, 2, 3):
        from_x.append(shift(turned, "x", -k % NX))
    mine = stacked((tokens, grad_out))
    left, right = shift(mine, "y", 1), shift(mine, "y", 3)
    plane = place_rows(x_at, from_x)
    fore = back = plane
    ring = [plane]
    for _ in range(3):
        fore, back = shift(fore, "z", 1), shift(back, "z", 7)
        ring += [fore, back]
    ring += [shift(fore[:half], "z", 1), shift(back[half:], "z", 7)]

    t_far, g_far = shift(left[0], "y", 1), shift(right[1], "y", 3)
    across_near = shift(stacked((mine, right, left)), "c", 1)
    across_far = shift(stacked((t_far, g_far)), "c", 1)
    pieces = (mine, right, left, t_far, g_far, across_near, across_far)
    weights = place_rows(ring_at, ring)

    normed, g_all, inv_rms, hidden, pre_grads = forward(pieces, weights, gain_rows)
    factor = (rows * lax.axis_size(FS)) ** (-0.5)

    parts = weight_grads(table, normed, pre_grads, cols, factor, False)
    from_x = [shift(p, "x", k) for k, p in zip((1, 2, 3), parts[1:])]
    down = weight_grads(table, g_all, hidden, cols, 0.5 * factor, True)
    distances = (1, 7, 2, 6, 3, 5, 4)
    from_z = [shift(down[k], "z", k) for k in distances]
    near, far = input_grads(pieces, inv_rms, gain_rows, pre_grads, weights)
    across = shift(far, "c", 1)

    total, *to_y = pair_sums(near, across, grad_out)
    from_y = [shift(p, "y", DISTANCES[i]) for i, p in zip((1, 2, 3), to_y)]
    grad_input = final_sum(total, from_y)

    ordered = sum_over_x(table, (parts[0], *from_x))
    got_both = lax.all_to_all(ordered, "z", 0, 0, tiled=True)
    own_down, *for_x = sum_for_x(table, (down[0], *from_z), cols)
    x_down = [shift(p, "x", k) for k, p in zip((1, 2, 3), for_x)]
    peers = NZ * NX
    grad_down, down_squares = down_gradient(own_down, x_down)
    grad_gate, grad_up, spread = gradients(got_both, down_squares, peers)
    everything = lax.all_to_all(spread, FS, 0, 0, tiled=True)
    row_squares = mean_squares(everything, cols * peers)
    return (grad_input, grad_gate.T, grad_up.T, grad_down.T, row_squares)


def solution(mesh):
    split = Mesh(mesh.devices.reshape(NZ, NX, NY, 2), FS + TP)

    return jax.shard_map(
        on_device,
        mesh=split,
        in_specs=(P(FS, TP), P(FS, TP), P(), P(TP, FS), P(TP, FS), P(TP, FS)),
        out_specs=(P(FS, TP), P(TP, FS), P(TP, FS), P(TP, FS), P(None, TP)),
        check_vma=False,
    )
```

```python
import jax
import jax.numpy as jnp
from jax import lax
from jax.experimental import pallas as pl
from jax.experimental.pallas import tpu as pltpu
from jax.sharding import Mesh
from jax.sharding import PartitionSpec as P

FS = ("z", "x")
TP = ("y", "c")
NZ, NX, NY = 8, 4, 4
DISTANCES = (0, 1, 3, 2)
VMEM = pl.BlockSpec(memory_space=pltpu.VMEM)
SMEM = pl.BlockSpec(memory_space=pltpu.SMEM)


def shift(x, axis, k):
    n = lax.axis_size(axis)
    return lax.ppermute(x, axis, [(i, (i + k) % n) for i in range(n)])


def local_kernel(body, out, ins, flops=1 << 20, limit=4, scratch=()):
    size = sum(a.size * a.dtype.itemsize for a in ins[1:])
    return pl.pallas_call(
        body,
        out_shape=out,
        in_specs=[SMEM] + [VMEM] * (len(ins) - 1),
        out_specs=jax.tree.map(lambda _: VMEM, out),
        scratch_shapes=scratch,
        cost_estimate=pl.CostEstimate(flops=flops, bytes_accessed=2 * size, transcendentals=0),
        compiler_params=pltpu.CompilerParams(vmem_limit_bytes=limit << 20),
    )(*ins)


def place_rows(places, pieces):
    rows = sum(p.shape[0] for p in pieces)

    def body(at, *refs):
        out = refs[-1]
        for k, ref in enumerate(refs[:-1]):
            start = pl.multiple_of(at[k], 64)
            out[pl.ds(start, ref.shape[0]), :] = ref[...]

    out = jax.ShapeDtypeStruct((rows, pieces[0].shape[1]), pieces[0].dtype)
    return local_kernel(body, out, (places, *pieces))


def place_down(table, pieces):
    _, cols, hid = pieces[0].shape

    def body(at, *refs):
        def step(b, carry):
            for k in range(NX):
                first = at[b] * (NX * cols) + ((at[NZ] + k) & 3) * cols
                refs[-1][pl.ds(pl.multiple_of(first, cols), cols), :] = refs[k][b]
            return carry

        lax.fori_loop(0, NZ, step, 0)

    out = jax.ShapeDtypeStruct((NZ * NX * cols, hid), pieces[0].dtype)
    return local_kernel(body, out, (table, *pieces))


def ordered_gain(block_at, gain):
    blocks, width = gain.shape

    def body(at, ref, out):
        for r in range(blocks):
            out[:, r * width : (r + 1) * width] = ref[pl.ds(at[r], 1), :]

    out = jax.ShapeDtypeStruct((1, blocks * width), gain.dtype)
    return local_kernel(body, out, (block_at, gain))


def sum_over_x(table, terms):
    def body(at, *refs):
        def step(i, carry):
            here = pl.ds(pl.multiple_of(i * 16, 16), 16)
            for b in range(NZ):
                total = refs[0][at[b], here, :].astype(jnp.float32)
                for ref in refs[1:-1]:
                    total += ref[at[b], here, :].astype(jnp.float32)
                refs[-1][b, here, :] = total.astype(refs[-1].dtype)
            return carry

        lax.fori_loop(0, terms[0].shape[1] // 16, step, 0)

    out = jax.ShapeDtypeStruct(terms[0].shape, terms[0].dtype)
    return local_kernel(body, out, (table, *terms))


def weight_grads(table, left, right, cols, scale, by_z):
    width, hid = left.shape[1] // NZ, right.shape[1]

    def body(at, l_ref, r_ref, *refs):
        scratch = refs[-1]

        def block(r):
            lanes = pl.ds(pl.multiple_of(r * width, width), width)
            product = lax.dot_general(
                l_ref[:, lanes],
                r_ref[...],
                (((0,), (0,)), ((), ())),
                preferred_element_type=jnp.float32,
            )
            term = (scale * product).astype(jnp.bfloat16)
            if by_z:
                scratch[r] = term
            else:
                scratch[r & 1] = term
                for k in range(NX):
                    first = pl.multiple_of(((at[NZ] + k) & 3) * cols, cols)
                    refs[k][r] = scratch[r & 1, pl.ds(first, cols), :]

        def step(i, carry):
            block(2 * i)
            block(2 * i + 1)
            return carry

        lax.fori_loop(0, NZ // 2, step, 0)
        if by_z:
            for j in range(NZ):
                refs[j][...] = scratch[at[NZ + 1 + j]]

    if by_z:
        out = tuple(jax.ShapeDtypeStruct((width, hid), jnp.bfloat16) for _ in range(NZ))
        scratch = [pltpu.VMEM((NZ, width, hid), jnp.bfloat16)]
    else:
        out = tuple(jax.ShapeDtypeStruct((NZ, cols, hid), jnp.bfloat16) for _ in range(NX))
        scratch = [pltpu.VMEM((2, width, hid), jnp.bfloat16)]
    flops = 2 * left.size * hid
    return local_kernel(body, out, (table, left, right), flops, 12, scratch)


def stacked(pieces):
    counts = [p.shape[0] if p.ndim == 3 else 1 for p in pieces]

    def body(at, *refs):
        place = 0
        for ref, n in zip(refs[:-1], counts):
            for k in range(n):
                refs[-1][place + k] = ref[k] if len(ref.shape) == 3 else ref[...]
            place += n

    out = jax.ShapeDtypeStruct((sum(counts), *pieces[0].shape[-2:]), pieces[0].dtype)
    return local_kernel(body, out, (jnp.zeros((1,), jnp.int32), *pieces), limit=6)


def block_rows(refs, kind, block, here):
    if block < 3:
        return refs[block][kind, here, :]
    if block == 3:
        return refs[3 + kind][here, :]
    if block < 7:
        return refs[5][(block - 4) * 2 + kind, here, :]
    return refs[6][kind, here, :]


TILE = 256


def forward(pieces, weights, down_w, gain_rows):
    rows, width = pieces[3].shape
    blocks = gain_rows.shape[1] // width
    hid = down_w.shape[1]

    def body(at, *refs):
        p_refs, (w_ref, d_ref, gain_ref) = refs[:7], refs[7:10]
        normed, g_all, inv_ref, hidden, pre_grads = refs[10:]

        def step(i, carry):
            start = pl.multiple_of(i * TILE, TILE)
            here = pl.ds(start, TILE)
            squares = jnp.zeros((TILE, width), jnp.float32)
            for r in range(blocks):
                t = block_rows(p_refs, 0, r, here).astype(jnp.float32)
                squares += t * t
            mean = jnp.sum(squares, axis=-1, keepdims=True) / (blocks * width)
            inv = lax.rsqrt(mean + 1e-06)
            inv_ref[here, :] = inv
            for r in range(blocks):
                lanes = slice(r * width, (r + 1) * width)
                t = block_rows(p_refs, 0, r, here).astype(jnp.float32)
                normed[here, lanes] = (t * inv * gain_ref[:, lanes]).astype(jnp.bfloat16)
                g_all[here, lanes] = block_rows(p_refs, 1, r, here)
            both = jnp.dot(normed[here, :], w_ref[...], preferred_element_type=jnp.float32)
            grad_hidden = 0.5 * jnp.dot(
                g_all[here, :], d_ref[...], preferred_element_type=jnp.float32
            )
            gate_pre, up_pre = both[:, :hid], both[:, hid:]
            sigma = jax.nn.sigmoid(gate_pre)
            active = gate_pre * sigma
            hidden[here, :] = (active * up_pre).astype(jnp.bfloat16)
            slope = sigma * (1.0 + gate_pre * (1.0 - sigma))
            pre_grads[here, :hid] = (grad_hidden * up_pre * slope).astype(jnp.bfloat16)
            pre_grads[here, hid:] = (grad_hidden * active).astype(jnp.bfloat16)
            return carry

        lax.fori_loop(0, rows // TILE, step, 0)

    half = jnp.bfloat16
    out = (
        jax.ShapeDtypeStruct((rows, blocks * width), half),
        jax.ShapeDtypeStruct((rows, blocks * width), half),
        jax.ShapeDtypeStruct((rows, 1), jnp.float32),
        jax.ShapeDtypeStruct((rows, hid), half),
        jax.ShapeDtypeStruct((rows, 2 * hid), half),
    )
    ins = (jnp.zeros((1,), jnp.int32), *pieces, weights, down_w, gain_rows)
    return local_kernel(body, out, ins, 5 * 10**9, 12)


def input_grads(pieces, inv_rms, gain_rows, pre_grads, weights):
    rows, width = pieces[3].shape
    blocks = gain_rows.shape[1] // width
    near = blocks // 2 * width

    def body(at, *refs):
        t_refs, (inv_ref, gain_ref, p_ref, w_ref) = refs[:7], refs[7:11]
        outs, acc = refs[11:13], refs[13]

        def step(i, carry):
            start = pl.multiple_of(i * TILE, TILE)
            here = pl.ds(start, TILE)
            acc[...] = lax.dot_general(
                p_ref[here, :],
                w_ref[...],
                (((1,), (1,)), ((), ())),
                preferred_element_type=jnp.float32,
            )
            inv = inv_ref[here, :]
            inner = jnp.zeros((TILE, width), jnp.float32)
            for r in range(blocks):
                lanes = slice(r * width, (r + 1) * width)
                unit = block_rows(t_refs, 0, r, here).astype(jnp.float32) * inv
                inner += gain_ref[:, lanes] * acc[:, lanes] * unit
            mean = jnp.sum(inner, axis=-1, keepdims=True) / (blocks * width)
            for r in range(blocks):
                lanes = slice(r * width, (r + 1) * width)
                unit = block_rows(t_refs, 0, r, here).astype(jnp.float32) * inv
                value = inv * (gain_ref[:, lanes] * acc[:, lanes] - unit * mean)
                place = slice(r % 4 * width, (r % 4 + 1) * width)
                outs[r // 4][here, place] = value.astype(jnp.bfloat16)
            return carry

        lax.fori_loop(0, rows // TILE, step, 0)

    out = tuple(jax.ShapeDtypeStruct((rows, near), jnp.bfloat16) for _ in range(2))
    ins = (jnp.zeros((1,), jnp.int32), *pieces, inv_rms, gain_rows, pre_grads, weights)
    scratch = [pltpu.VMEM((TILE, blocks * width), jnp.float32)]
    return local_kernel(body, out, ins, 3 * 10**9, 12, scratch)


def sum_for_x(table, terms, cols):
    hid = terms[0].shape[1]

    def body(at, *refs):
        outs = refs[NZ:]

        def step(i, carry):
            here = pl.ds(pl.multiple_of(i * 16, 16), 16)
            for k in range(NX):
                first = pl.multiple_of(((at[NZ] + k) & 3) * cols + i * 16, 16)
                total = refs[0][pl.ds(first, 16), :].astype(jnp.float32)
                for ref in refs[1:NZ]:
                    total += ref[pl.ds(first, 16), :].astype(jnp.float32)
                outs[k][here, :] = total.astype(outs[k].dtype)
            return carry

        lax.fori_loop(0, cols // 16, step, 0)

    out = (jax.ShapeDtypeStruct((cols, hid), jnp.float32),)
    out += tuple(jax.ShapeDtypeStruct((cols, hid), terms[0].dtype) for _ in range(NX - 1))
    return local_kernel(body, out, (table, *terms))


def kernel(body, out, ins, specs, scratch=(), limit=4):
    size = sum(a.size * a.dtype.itemsize for a in ins)
    return pl.pallas_call(
        body,
        out_shape=out,
        in_specs=specs,
        out_specs=jax.tree.map(lambda _: VMEM, out),
        scratch_shapes=scratch,
        cost_estimate=pl.CostEstimate(flops=1 << 20, bytes_accessed=2 * size, transcendentals=0),
        compiler_params=pltpu.CompilerParams(vmem_limit_bytes=limit << 20),
    )(*ins)


def pair_sums(near, across, grad_out):
    rows, width = grad_out.shape

    def body(near_ref, across_ref, grad_ref, *outs):
        def step(n, carry):
            here = pl.ds(pl.multiple_of(n * TILE, TILE), TILE)
            for i, out in enumerate(outs):
                lanes = slice(i * width, (i + 1) * width)
                both = near_ref[here, lanes].astype(jnp.float32)
                both += across_ref[here, lanes].astype(jnp.float32)
                if i == 0:
                    both += grad_ref[here, :].astype(jnp.float32)
                out[here, :] = both.astype(out.dtype)
            return carry

        lax.fori_loop(0, rows // TILE, step, 0)

    out = (jax.ShapeDtypeStruct((rows, width), jnp.float32),)
    out += tuple(jax.ShapeDtypeStruct((rows, width), jnp.bfloat16) for _ in range(3))
    return kernel(body, out, (near, across, grad_out), [VMEM] * 3, limit=12)


def final_sum(total, arrived):
    def body(total_ref, *refs):
        def step(n, carry):
            here = pl.ds(pl.multiple_of(n * TILE, TILE), TILE)
            both = total_ref[here, :]
            for ref in refs[:-1]:
                both += ref[here, :].astype(jnp.float32)
            refs[-1][here, :] = both.astype(jnp.bfloat16)
            return carry

        lax.fori_loop(0, total.shape[0] // TILE, step, 0)

    ins = (total, *arrived)
    out = jax.ShapeDtypeStruct(total.shape, jnp.bfloat16)
    return kernel(body, out, ins, [VMEM] * len(ins), limit=12)


def down_gradient(own, arrived):
    def body(own_ref, *refs):
        total = own_ref[...]
        for piece in refs[:-2]:
            total += piece[...].astype(jnp.float32)
        refs[-2][...] = total
        refs[-1][...] = jnp.sum(total * total, axis=0, keepdims=True)

    out = (
        jax.ShapeDtypeStruct(own.shape, jnp.float32),
        jax.ShapeDtypeStruct((1, own.shape[1]), jnp.float32),
    )
    ins = (own, *arrived)
    return kernel(body, out, ins, [VMEM] * len(ins))


def gradients(got, down_squares, peers):
    _, cols, both = got.shape
    hid = both // 2

    def body(ref, down_ref, gate, up, spread, line, sem):
        copy = pltpu.make_async_copy(down_ref, line.at[:, both:], sem)
        copy.start()
        for i, out in enumerate((gate, up)):
            lanes = slice(i * hid, (i + 1) * hid)
            total = ref[0, :, lanes].astype(jnp.float32)
            for b in range(1, NZ):
                total += ref[b, :, lanes].astype(jnp.float32)
            out[...] = total
            line[:, lanes] = jnp.sum(total * total, axis=0, keepdims=True)
        copy.wait()
        for k in range(peers):
            spread[k] = line[...]

    out = tuple(jax.ShapeDtypeStruct((cols, hid), jnp.float32) for _ in range(2))
    out += (jax.ShapeDtypeStruct((peers, 1, both + hid), jnp.float32),)
    specs = [VMEM, pl.BlockSpec(memory_space=pl.ANY)]
    scratch = [pltpu.VMEM((1, both + hid), jnp.float32), pltpu.SemaphoreType.DMA]
    return kernel(body, out, (got, down_squares), specs, scratch)


def mean_squares(everything, columns):
    peers, _, width = everything.shape
    hid = width // 3

    def body(ref, out):
        total = ref[0]
        for k in range(1, peers):
            total += ref[k]
        for i in range(3):
            out[i : i + 1, :] = total[:, i * hid : (i + 1) * hid] / columns

    out = jax.ShapeDtypeStruct((3, hid), jnp.float32)
    return kernel(body, out, (everything,), [VMEM])


def on_device(tokens, grad_out, norm_gain, gate_weight, up_weight, down_weight):
    z, x, y, c = (lax.axis_index(a) for a in ("z", "x", "y", "c"))
    rows, width = tokens.shape
    hid, cols = gate_weight.shape
    eight, four = jnp.arange(NZ, dtype=jnp.int32), jnp.arange(NX, dtype=jnp.int32)

    def slot_of(block):
        dy = ((block >> 1) - y) & 3
        return (((block & 1) ^ c) << 2) + (dy ^ (dy >> 1))

    block_at = ((y + ((eight & 3) ^ ((eight & 3) >> 1))) & 3) * 2 + ((eight >> 2) ^ c)
    slots = slot_of(eight)

    ring_steps = (0, -1, 1, -2, 2, -3, 3, 4, 4)
    height, half = NX * cols, NX * cols // 2
    ring_at = slot_of((z + jnp.array(ring_steps, jnp.int32)) & 7) * height
    ring_at = ring_at + jnp.array((0,) * 8 + (half,), jnp.int32)
    x_at = ((x + four) & 3) * cols
    table = jnp.concatenate([slots, x[None].astype(jnp.int32), slot_of((z + eight) & 7)])
    turned = jnp.concatenate([gate_weight, up_weight], axis=0).T
    down_own = jnp.broadcast_to(down_weight.T[None], (NZ, cols, hid))
    gain_table = norm_gain.reshape(NZ, width)
    gain_rows = ordered_gain(block_at, gain_table)
    ring_at, x_at, table, gain_rows, tokens, grad_out = lax.optimization_barrier(
        (ring_at, x_at, table, gain_rows, tokens, grad_out)
    )

    from_x = [turned]
    for k in (1, 2, 3):
        from_x.append(shift(turned, "x", -k % NX))
    mine = stacked((tokens, grad_out))
    left, right = shift(mine, "y", 1), shift(mine, "y", 3)
    down_z = lax.all_to_all(down_own, "z", 0, 0, tiled=True)
    plane = place_rows(x_at, from_x)
    down_x = [shift(down_z, "x", -k % NX) for k in (1, 2, 3)]
    fore = back = plane
    ring = [plane]
    for _ in range(3):
        fore, back = shift(fore, "z", 1), shift(back, "z", 7)
        ring += [fore, back]
    ring += [shift(fore[:half], "z", 1), shift(back[half:], "z", 7)]

    t_near, g_near = left[0], right[1]
    t_far, g_far = shift(t_near, "y", 1), shift(g_near, "y", 3)
    across_near = shift(stacked((mine, right, left)), "c", 1)
    across_far = shift(stacked((t_far, g_far)), "c", 1)
    pieces = (mine, right, left, t_far, g_far, across_near, across_far)
    down_w = place_down(table, (down_z, *down_x))
    weights = place_rows(ring_at, ring)

    normed, g_all, inv_rms, hidden, pre_grads = forward(pieces, weights, down_w, gain_rows)
    factor = (rows * lax.axis_size(FS)) ** (-0.5)

    parts = weight_grads(table, normed, pre_grads, cols, factor, False)
    from_x = [shift(p, "x", k) for k, p in zip((1, 2, 3), parts[1:])]
    down = weight_grads(table, g_all, hidden, cols, 0.5 * factor, True)
    distances = (1, 7, 2, 6, 3, 5, 4)
    from_z = [shift(down[k], "z", k) for k in distances]
    near, far = input_grads(pieces, inv_rms, gain_rows, pre_grads, weights)
    across = shift(far, "c", 1)

    total, *to_y = pair_sums(near, across, grad_out)
    from_y = [shift(p, "y", DISTANCES[i]) for i, p in zip((1, 2, 3), to_y)]
    grad_input = final_sum(total, from_y)

    ordered = sum_over_x(table, (parts[0], *from_x))
    got_both = lax.all_to_all(ordered, "z", 0, 0, tiled=True)
    own_down, *for_x = sum_for_x(table, (down[0], *from_z), cols)
    x_down = [shift(p, "x", k) for k, p in zip((1, 2, 3), for_x)]
    peers = NZ * NX
    grad_down, down_squares = down_gradient(own_down, x_down)
    grad_gate, grad_up, spread = gradients(got_both, down_squares, peers)
    everything = lax.all_to_all(spread, FS, 0, 0, tiled=True)
    row_squares = mean_squares(everything, cols * peers)
    return (grad_input, grad_gate.T, grad_up.T, grad_down.T, row_squares)


def solution(mesh):
    split = Mesh(mesh.devices.reshape(NZ, NX, NY, 2), FS + TP)

    return jax.shard_map(
        on_device,
        mesh=split,
        in_specs=(P(FS, TP), P(FS, TP), P(), P(TP, FS), P(TP, FS), P(TP, FS)),
        out_specs=(P(FS, TP), P(TP, FS), P(TP, FS), P(TP, FS), P(None, TP)),
        check_vma=False,
    )
```
